512 devices in a mesh: sp: 256 (over z, y, x), tp: 2 (over core).
Axes of the slice: x: 4, y: 8, z: 8, core: 2. Of those that a mesh axis runs over, the one named last changes fastest.
Arguments:
- proj_a: bfloat16 [65536, 3072], P('sp', 'tp'), may hold values from -20 to 20
- proj_gate: bfloat16 [65536, 3072], P('sp', 'tp'), may hold values from -6 to 6
- taps: bfloat16 [31, 3072], P(None, 'tp'), may hold values from -1 to 1
- norm_gain: float32 [3072], P('tp'), may hold values from 0.1 to 1.9
- norm_shift: float32 [3072], P('tp'), may hold values from -3 to 3
- cotangent: bfloat16 [65536, 3072], P('sp', 'tp'), may hold values from -6 to 6
Outputs:
- a_grad: bfloat16 [65536, 3072], P('sp', 'tp')
- gate_grad: bfloat16 [65536, 3072], P('sp', 'tp')
- taps_grad: float32 [31, 3072], P(None, 'tp')
- gain_grad: float32 [3072], P('tp')
- shift_grad: float32 [3072], P('tp')
The draws below stay inside these ranges and needn't reach their ends.
All inputs are finite; a program needn't handle non-finite values.
Results may differ from the reference program's by a relative error of at most 0.0048.
Values may be sent and summed in bfloat16 or wider, within the bound.
A program may use at most 64 MiB of HBM per device.

```python
import jax
import jax.numpy as jnp
from jax import lax

D = 3072
K = 31
TOK_DEV = 256
TOKENS = 65536
N_SP = 256


def draw_proj_a(key, part):
    first_key, second_key, third_key = jax.random.split(jax.random.fold_in(key, 17), 3)
    groups = jnp.arange(D) * 24 // D
    factors = jnp.exp(jax.random.uniform(second_key, (24,), jnp.float32, -1.1, 1.1))
    col_scale = factors[groups]
    row_groups = jnp.arange(TOKENS) * 64 // TOKENS
    row_factors = jnp.exp(jax.random.uniform(third_key, (64,), jnp.float32, -0.5, 0.5))
    row_scale = row_factors[row_groups]
    base = jax.random.truncated_normal(first_key, -4.0, 4.0, (TOKENS, D), jnp.float32)
    return (base * col_scale[None, :] * row_scale[:, None]).astype(jnp.bfloat16)


def level_of(own_key, dims, cuts, least, high):
    factor_of, own = 1.0, jax.random.fold_in(own_key, 6)
    for axis_at, parts in cuts:
        steps = jnp.exp(jax.random.uniform(jax.random.fold_in(own, axis_at), (parts,), jnp.float32, least / len(cuts), high / len(cuts)))
        factor_of = factor_of * jnp.repeat(steps, dims[axis_at] // parts).reshape([-1 if axis == axis_at else 1 for axis in range(len(dims))])
    return factor_of


def centred(key, extent, scale, most, shards=(), kind=jnp.bfloat16):
    entries = scale * jax.random.normal(key, extent, jnp.float32)
    if shards:
        entries = entries * level_of(key, extent, shards, -0.22, 0.18)
    return jnp.clip(entries, -most, most).astype(kind)


def setup_inputs(seed: int = 0) -> dict:
    key_of = jax.random.split(jax.random.key(seed), 7)
    return {
        "proj_a": draw_proj_a(jax.random.fold_in(key_of[6], 71), 0),
        "proj_gate": centred(key_of[1], (TOKENS, D), 1.5, 6.0, ((0, 256), (1, 2))),
        "taps": centred(key_of[2], (K, D), K ** -0.5, 1.0, ((1, 2),)),
        "norm_gain": jnp.clip(1.0 + 0.18 * jax.random.normal(key_of[3], (D,), jnp.float32), 0.1, 1.9),
        "norm_shift": centred(key_of[4], (D,), 0.5, 3.0, ((0, 2),), jnp.float32),
        "cotangent": centred(key_of[5], (TOKENS, D), 1.0, 6.0, ((0, 256), (1, 2))),
    }


EPS = 1e-05

def reference(proj_a, proj_gate, taps, norm_gain, norm_shift, cotangent):
    width = taps.shape[0]
    edge = width - 1
    rows = TOK_DEV
    blocks = N_SP
    gate_f = proj_gate.astype(jnp.float32)
    glu = (proj_a.astype(jnp.float32) * jax.nn.sigmoid(gate_f)).astype(jnp.bfloat16)
    glu_pad = jnp.concatenate([jnp.zeros((edge, D), jnp.bfloat16), glu], axis=0)
    tapf = taps.astype(jnp.float32)
    gain = norm_gain.astype(jnp.float32)
    shift = norm_shift.astype(jnp.float32)

    def first(index):
        start = index * rows
        ext = lax.dynamic_slice_in_dim(glu_pad, start, rows + edge, 0).astype(jnp.float32)
        cot = lax.dynamic_slice_in_dim(cotangent, start, rows, 0).astype(jnp.float32)
        conv = jnp.zeros((rows, D), jnp.float32)
        for k in range(width):
            conv = conv + tapf[k] * ext[k:k + rows]
        mean = lax.optimization_barrier(jnp.mean(conv, axis=1, keepdims=True))
        cent = conv - mean
        spread = lax.optimization_barrier(jnp.mean(cent * cent, axis=1, keepdims=True))
        rstd = lax.rsqrt(spread + EPS)
        normed = cent * rstd
        pre = normed * gain + shift
        sig = jax.nn.sigmoid(pre)
        dpre = cot * sig * (1.0 + pre * (1.0 - sig))
        dnormed = dpre * gain
        dconv = rstd * (dnormed - lax.optimization_barrier(jnp.mean(dnormed, axis=1, keepdims=True)) - normed * lax.optimization_barrier(jnp.mean(dnormed * normed, axis=1, keepdims=True)))
        return (dconv, lax.optimization_barrier(jnp.sum(dpre * normed, axis=0)), lax.optimization_barrier(jnp.sum(dpre, axis=0)))
    index = jnp.arange(blocks, dtype=jnp.int32)
    dconv_all, gain_parts, shift_parts = lax.map(first, index)
    dconv_pad = jnp.concatenate([dconv_all.reshape(blocks * rows, D), jnp.zeros((edge, D), jnp.float32)], axis=0)

    def second(index):
        start = index * rows
        dext = lax.dynamic_slice_in_dim(dconv_pad, start, rows + edge, 0)
        ext = lax.dynamic_slice_in_dim(glu_pad, start, rows + edge, 0).astype(jnp.float32)
        own = dext[:rows]
        dglu = jnp.zeros((rows, D), jnp.float32)
        for k in range(width):
            dglu = dglu + tapf[edge - k] * dext[k:k + rows]
        taps_part = jnp.stack([lax.optimization_barrier(jnp.sum(own * ext[j:j + rows], axis=0)) for j in range(width)])
        a_rows = lax.dynamic_slice_in_dim(proj_a, start, rows, 0).astype(jnp.float32)
        g_rows = lax.dynamic_slice_in_dim(gate_f, start, rows, 0)
        sg = jax.nn.sigmoid(g_rows)
        return ((dglu * sg).astype(jnp.bfloat16), (dglu * a_rows * sg * (1.0 - sg)).astype(jnp.bfloat16), taps_part)
    a_parts, gate_parts, taps_parts = lax.map(second, index)
    a_grad = a_parts.reshape(blocks * rows, D)
    gate_grad = gate_parts.reshape(blocks * rows, D)
    return (a_grad, gate_grad, lax.optimization_barrier(jnp.sum(taps_parts, axis=0)), lax.optimization_barrier(jnp.sum(gain_parts, axis=0)), lax.optimization_barrier(jnp.sum(shift_parts, axis=0)))
```

```python
import functools

import jax
import jax.numpy as jnp
from jax import lax
from jax.experimental import pallas as pl
from jax.experimental.pallas import tpu as pltpu
from jax.sharding import Mesh
from jax.sharding import PartitionSpec as P

SP = ("sp_0", "sp_1", "sp_2")
EPS = 1e-05
F32 = jnp.float32
BF16 = jnp.bfloat16
MESH = pl.DeviceIdType.MESH
S = 16
LANES = 128
ROWS = 256
EDGE = 30
TAPS = 31


def sigmoid(x):
    return 0.5 * jnp.tanh(0.5 * x) + 0.5


def kernel(
    sizes,
    a_hbm,
    g_hbm,
    cot_hbm,
    taps_ref,
    gain_ref,
    shift_ref,
    ag_hbm,
    gg_hbm,
    tg_ref,
    gng_ref,
    shg_ref,
    a_in,
    g_in,
    cot_in,
    a_tail,
    g_tail,
    ap,
    sg,
    cotp,
    ext,
    dce,
    tapb,
    convs,
    dnorm,
    rowsum,
    rowdot,
    mean_l,
    rstd_s,
    m1_s,
    m2_s,
    stat_snd,
    stat_rcv,
    sums_snd,
    sums_rcv,
    halo_snd,
    halo_rcv,
    halo_f,
    back_f,
    back_snd,
    back_rcv,
    col,
    red,
    part,
    part_rcv,
    line_snd,
    line_rcv,
    full_snd,
    full_rcv,
    ag_out,
    gg_out,
    in_sem,
    out_sem,
    tp_send,
    tp_recv,
    halo_send,
    halo_recv,
    red_send,
    red_recv,
):
    nz, ny, nx = sizes
    blocks = ext.shape[0]
    chans = blocks * LANES
    plane = nz * ny
    z, y, x, core = (lax.axis_index(name) for name in (*SP, "tp"))
    sp = (z * ny + y) * nx + x
    total = plane * nx

    def place(index):
        return (index // (ny * nx), index // nx % ny, index % nx, core)

    after = place(lax.rem(sp + 1, total))
    behind = place(lax.rem(sp + total - 1, total))
    other = (z, y, x, 1 - core)
    mine = z * ny + y

    def in_plane(j):
        pz = lax.rem(z + j // ny, nz)
        py = lax.rem(y + j % ny, ny)
        return pz * ny + py, (pz, py, x, core)

    def in_line(j):
        return (z, y, lax.rem(x + j, nx), core)

    tail = pl.ds(ROWS - 32, 32)
    loads = [
        pltpu.make_async_copy(a_hbm.at[tail], a_tail, in_sem.at[0]),
        pltpu.make_async_copy(g_hbm.at[tail], g_tail, in_sem.at[1]),
        pltpu.make_async_copy(a_hbm, a_in, in_sem.at[2]),
        pltpu.make_async_copy(g_hbm, g_in, in_sem.at[3]),
        pltpu.make_async_copy(cot_hbm, cot_in, in_sem.at[4]),
    ]
    for load in loads:
        load.start()

    barrier = pltpu.get_barrier_semaphore()

    def greet(device):
        pl.semaphore_signal(barrier, inc=1, device_id=device, device_id_type=MESH)

    greet(other)
    greet(after)
    greet(behind)

    @pl.loop(1, nx)
    def _(j):
        greet(in_line(j))

    @pl.loop(1, plane)
    def _(j):
        greet(in_plane(j)[1])

    loads[0].wait()
    loads[1].wait()
    for c in range(blocks):
        lanes = pl.ds(c * LANES, LANES)
        halo_snd[c] = (a_tail[:, lanes].astype(F32) * sigmoid(g_tail[:, lanes].astype(F32))).astype(BF16)

    pl.semaphore_wait(barrier, 3 + (nx - 1) + (plane - 1))
    halo = pltpu.make_async_remote_copy(
        halo_snd, halo_rcv, halo_send.at[0], halo_recv.at[0], device_id=after, device_id_type=MESH
    )
    halo.start()

    for c in range(blocks):
        rows = taps_ref[:, c * LANES : (c + 1) * LANES].astype(F32)
        for k in range(TAPS):
            tapb[c, k] = jnp.broadcast_to(rows[k : k + 1], (S, LANES)).astype(BF16)

    at = lax.broadcasted_iota(jnp.int32, (ROWS, ROWS), 0)
    pos = lax.broadcasted_iota(jnp.int32, (ROWS, ROWS), 1)
    perm = jnp.where(pos == (at % S) * S + at // S, 1.0, 0.0).astype(BF16)
    loads[2].wait()
    loads[3].wait()
    loads[4].wait()

    def moved(v):
        return jnp.dot(perm, v, preferred_element_type=F32)

    @pl.loop(0, blocks // 2)
    def _(cc):
        wide = pl.ds(pl.multiple_of(cc * 2 * LANES, 2 * LANES), 2 * LANES)
        av = moved(a_in[:, wide])
        sv = sigmoid(moved(g_in[:, wide]))
        glu = (av * sv).astype(BF16)
        cv = moved(cot_in[:, wide])
        for h in range(2):
            lanes = slice(h * LANES, (h + 1) * LANES)
            c = cc * 2 + h
            ap[c] = av[:, lanes].astype(BF16)
            sg[c] = sv[:, lanes]
            cotp[c] = cv[:, lanes].astype(BF16)
            for r in range(S):
                ext[c, EDGE + r] = glu[r * S : (r + 1) * S, lanes]

    halo.wait_recv()
    row = lax.broadcasted_iota(jnp.int32, (S, LANES), 0)

    @pl.loop(0, blocks)
    def _(c):
        halo_f[c] = jnp.where(sp > 0, halo_rcv[c].astype(F32), 0.0)

    @pl.loop(0, blocks)
    def _(c):
        for r in range(S):
            v = ext[c, EDGE + r].astype(F32)
            one = jnp.where(row == 0, halo_f[c, S + r : S + r + 1], pltpu.roll(v, 1, 0))
            ext[c, EDGE - S + r] = one.astype(BF16)
            if r >= 2:
                two = jnp.where(row == 0, halo_f[c, r : r + 1], pltpu.roll(one, 1, 0))
                ext[c, r - 2] = two.astype(BF16)

    rowsum[...] = jnp.zeros_like(rowsum)

    @pl.loop(0, blocks)
    def _(c):
        for q in range(S // 4):
            acc = [None] * 4
            for k in range(TAPS):
                tap = tapb[c, k].astype(F32)
                for i in range(4):
                    v = ext[c, q * 4 + i + k].astype(F32) * tap
                    acc[i] = v if acc[i] is None else acc[i] + v
            for i in range(4):
                convs[c, q * 4 + i] = acc[i]
                rowsum[q * 4 + i] += acc[i]

    for r in range(S):
        mean_l[r] = jnp.broadcast_to(jnp.sum(rowsum[r], axis=1, keepdims=True) / chans, (S, LANES))

    @pl.loop(0, S)
    def _(r):
        m = mean_l[r]
        acc = jnp.zeros((S, LANES), F32)
        for c in range(blocks):
            cent = convs[c, r] - m
            acc = acc + cent * cent
        rowdot[r] = acc

    lane = lax.broadcasted_iota(jnp.int32, (S, LANES), 1)
    for r in range(S):
        stat_snd[r] = jnp.where(lane == 0, mean_l[r], jnp.sum(rowdot[r], axis=1, keepdims=True))
    stat = pltpu.make_async_remote_copy(
        stat_snd, stat_rcv, tp_send.at[0], tp_recv.at[0], device_id=other, device_id_type=MESH
    )
    stat.start()
    stat.wait()
    for r in range(S):
        own_m, far_m = mean_l[r], jnp.broadcast_to(stat_rcv[r][:, 0:1], (S, LANES))
        own_q, far_q = stat_snd[r][:, 1:2], stat_rcv[r][:, 1:2]
        diff = own_m - far_m
        spread = (own_q + far_q + diff * diff * (chans / 2)) / (2 * chans)
        mean_l[r] = 0.5 * (own_m + far_m)
        rstd_s[r] = lax.rsqrt(spread + EPS)

    col[...] = jnp.zeros_like(col)

    @pl.loop(0, S)
    def _(r):
        m, rs = mean_l[r], rstd_s[r]
        acc1 = jnp.zeros((S, LANES), F32)
        acc2 = jnp.zeros((S, LANES), F32)
        for c in range(blocks):
            lanes = slice(c * LANES, (c + 1) * LANES)
            normed = (convs[c, r] - m) * rs
            gain = gain_ref[:, lanes]
            pre = normed * gain + shift_ref[:, lanes]
            sig = sigmoid(pre)
            cv = cotp[c, pl.ds(pl.multiple_of(r * S, S), S)].astype(F32)
            dpre = cv * sig * (1.0 + pre * (1.0 - sig))
            dn = dpre * gain
            convs[c, r] = normed
            dnorm[c, r] = dn
            acc1 = acc1 + dn
            acc2 = acc2 + dn * normed
            prod = dpre * normed
            col[c, 0] += prod[:8] + prod[8:]
            col[c, 1] += dpre[:8] + dpre[8:]
        rowsum[r] = acc1
        rowdot[r] = acc2

    for r in range(S):
        sums_snd[r] = jnp.where(
            lane == 0,
            jnp.sum(rowsum[r], axis=1, keepdims=True),
            jnp.sum(rowdot[r], axis=1, keepdims=True),
        )
    sums = pltpu.make_async_remote_copy(
        sums_snd, sums_rcv, tp_send.at[1], tp_recv.at[1], device_id=other, device_id_type=MESH
    )
    sums.start()
    sums.wait()
    for r in range(S):
        both = (sums_snd[r] + sums_rcv[r]) / (2 * chans)
        rs = rstd_s[r]
        m1_s[r] = rs * both[:, 0:1]
        m2_s[r] = rs * both[:, 1:2]

    @pl.loop(0, blocks)
    def _(c):
        for r in range(S):
            d = rstd_s[r] * dnorm[c, r] - m1_s[r] - convs[c, r] * m2_s[r]
            dce[c, r] = d.astype(BF16)
            back_f[c, r : r + 1] = d[0:1]
            back_f[c, S + r : S + r + 1] = d[1:2]
        back_snd[c] = back_f[c].astype(BF16)

    back = pltpu.make_async_remote_copy(
        back_snd, back_rcv, halo_send.at[1], halo_recv.at[1], device_id=behind, device_id_type=MESH
    )
    back.start()

    for extra in range(5 * blocks, part.shape[0]):
        part[extra] = jnp.zeros((8, LANES), BF16)

    @pl.loop(0, blocks)
    def _(c):
        for q in range(8):
            ks = [k for k in range(q * 4, q * 4 + 4) if k < TAPS]
            acc = [None] * len(ks)
            for r in range(S):
                d = dce[c, r].astype(F32)
                for i, k in enumerate(ks):
                    v = ext[c, k + r].astype(F32) * d
                    acc[i] = v if acc[i] is None else acc[i] + v
            for i, k in enumerate(ks):
                red[pl.ds(9 * k, 8), :] = acc[i][:8] + acc[i][8:]
        red[pl.ds(9 * TAPS, 8), :] = col[c, 0]
        for g in range(4):
            rows = red[pl.ds(72 * g, 8, stride=9), :]
            for s in range(1, 8):
                rows = rows + red[pl.ds(72 * g + s, 8, stride=9), :]
            part[5 * c + g] = rows.astype(BF16)
        part[5 * c + 4] = jnp.broadcast_to(jnp.sum(col[c, 1], axis=0, keepdims=True), (8, LANES)).astype(BF16)

    per = part.shape[0] // plane

    def shard(index):
        return pl.ds(index * per, per)

    def scatter(index, device):
        return pltpu.make_async_remote_copy(
            part.at[shard(index)],
            part_rcv.at[shard(mine)],
            red_send.at[0],
            red_recv.at[0],
            device_id=device,
            device_id_type=MESH,
        )

    @pl.loop(1, plane)
    def _(j):
        scatter(*in_plane(j)).start()

    part_rcv[shard(mine)] = part[shard(mine)]

    back.wait_recv()

    @pl.loop(0, blocks)
    def _(c):
        halo_f[c] = jnp.where(sp < total - 1, back_rcv[c].astype(F32), 0.0)

    @pl.loop(0, blocks)
    def _(c):
        for r in range(S):
            v = dce[c, r].astype(F32)
            one = jnp.where(row == S - 1, halo_f[c, r : r + 1], pltpu.roll(v, S - 1, 0))
            dce[c, S + r] = one.astype(BF16)
            if r < EDGE - S:
                two = jnp.where(row == S - 1, halo_f[c, S + r : S + r + 1], pltpu.roll(one, S - 1, 0))
                dce[c, 2 * S + r] = two.astype(BF16)

    @pl.loop(0, blocks)
    def _(c):
        for q in range(S // 4):
            acc = [None] * 4
            for k in range(TAPS):
                tap = tapb[c, k].astype(F32)
                for i in range(4):
                    v = dce[c, q * 4 + i + EDGE - k].astype(F32) * tap
                    acc[i] = v if acc[i] is None else acc[i] + v
            for i in range(4):
                convs[c, q * 4 + i] = acc[i]

    @pl.loop(0, blocks // 2)
    def _(cc):
        wide = pl.ds(pl.multiple_of(cc * 2 * LANES, 2 * LANES), 2 * LANES)
        da, dg = [], []
        for h in range(2):
            c = cc * 2 + h
            grad = convs[c].reshape(ROWS, LANES)
            sv = sg[c]
            first = grad * sv
            da.append(first.astype(BF16))
            dg.append((first * ap[c].astype(F32) * (1.0 - sv)).astype(BF16))
        ag_out[:, wide] = moved(jnp.concatenate(da, axis=1)).astype(BF16)
        gg_out[:, wide] = moved(jnp.concatenate(dg, axis=1)).astype(BF16)

    stores = [
        pltpu.make_async_copy(ag_out, ag_hbm, out_sem.at[0]),
        pltpu.make_async_copy(gg_out, gg_hbm, out_sem.at[1]),
    ]
    for store in stores:
        store.start()

    def wait_all(ref, count, size, sem):
        some = ref.at[pl.ds(0, count * size)]
        pltpu.make_async_copy(some, some, sem).wait()

    wait_all(part_rcv, plane - 1, per, red_recv.at[0])
    sums8 = part_rcv[pl.ds(0, per)].astype(F32)
    for j in range(1, plane):
        sums8 = sums8 + part_rcv[pl.ds(j * per, per)].astype(F32)
    line_snd[...] = sums8
    line_rcv[pl.ds(x * per, per)] = sums8

    def along(j):
        return pltpu.make_async_remote_copy(
            line_snd,
            line_rcv.at[shard(x)],
            red_send.at[1],
            red_recv.at[1],
            device_id=in_line(j),
            device_id_type=MESH,
        )

    @pl.loop(1, nx)
    def _(j):
        along(j).start()

    wait_all(line_rcv, nx - 1, per, red_recv.at[1])
    sums8 = line_rcv[pl.ds(0, per)]
    for j in range(1, nx):
        sums8 = sums8 + line_rcv[pl.ds(j * per, per)]
    full_snd[...] = sums8.astype(BF16)
    full_rcv[shard(mine)] = sums8.astype(BF16)

    def spread_out(j):
        return pltpu.make_async_remote_copy(
            full_snd,
            full_rcv.at[shard(mine)],
            red_send.at[2],
            red_recv.at[2],
            device_id=in_plane(j)[1],
            device_id_type=MESH,
        )

    @pl.loop(1, plane)
    def _(j):
        spread_out(j).start()

    wait_all(full_rcv, plane - 1, per, red_recv.at[2])
    for c in range(blocks):
        lanes = slice(c * LANES, (c + 1) * LANES)
        for g in range(4):
            rows = full_rcv[5 * c + g].astype(F32)
            if g < 3:
                tg_ref[8 * g : 8 * g + 8, lanes] = rows
            else:
                tg_ref[24:TAPS, lanes] = rows[:7]
                gng_ref[:, lanes] = rows[7:8]
        shg_ref[:, lanes] = full_rcv[5 * c + 4].astype(F32)[0:1]

    for store in stores:
        store.wait()
    halo.wait_send()
    back.wait_send()
    wait_all(part, plane - 1, per, red_send.at[0])
    wait_all(line_rcv, nx - 1, per, red_send.at[1])
    wait_all(full_rcv, plane - 1, per, red_send.at[2])


def body(sizes, proj_a, proj_gate, taps, norm_gain, norm_shift, cotangent):
    rows, chans = proj_a.shape
    blocks = chans // LANES
    nz, ny, nx = sizes
    plane = nz * ny
    per = -(-5 * blocks // plane)
    shards = per * plane
    any_space = pl.BlockSpec(memory_space=pl.ANY)
    vmem = pl.BlockSpec(memory_space=pltpu.VMEM)
    tile = (S, S, LANES)
    edge = (blocks, 32, LANES)
    outs = pl.pallas_call(
        functools.partial(kernel, sizes),
        out_shape=(
            jax.ShapeDtypeStruct((rows, chans), BF16),
            jax.ShapeDtypeStruct((rows, chans), BF16),
            jax.ShapeDtypeStruct((TAPS, chans), F32),
            jax.ShapeDtypeStruct((1, chans), F32),
            jax.ShapeDtypeStruct((1, chans), F32),
        ),
        in_specs=[any_space] * 3 + [vmem] * 3,
        out_specs=(any_space, any_space, vmem, vmem, vmem),
        scratch_shapes=[
            pltpu.VMEM((rows, chans), BF16),
            pltpu.VMEM((rows, chans), BF16),
            pltpu.VMEM((rows, chans), BF16),
            pltpu.VMEM((32, chans), BF16),
            pltpu.VMEM((32, chans), BF16),
            pltpu.VMEM((blocks, rows, LANES), BF16),
            pltpu.VMEM((blocks, rows, LANES), F32),
            pltpu.VMEM((blocks, rows, LANES), BF16),
            pltpu.VMEM((blocks, EDGE + S, S, LANES), BF16),
            pltpu.VMEM((blocks, EDGE + S, S, LANES), BF16),
            pltpu.VMEM((blocks, TAPS, S, LANES), BF16),
            pltpu.VMEM((blocks, *tile), F32),
            pltpu.VMEM((blocks, *tile), F32),
            pltpu.VMEM(tile, F32),
            pltpu.VMEM(tile, F32),
            pltpu.VMEM(tile, F32),
            pltpu.VMEM(tile, F32),
            pltpu.VMEM(tile, F32),
            pltpu.VMEM(tile, F32),
            pltpu.VMEM(tile, F32),
            pltpu.VMEM(tile, F32),
            pltpu.VMEM(tile, F32),
            pltpu.VMEM(tile, F32),
            pltpu.VMEM(edge, BF16),
            pltpu.VMEM(edge, BF16),
            pltpu.VMEM(edge, F32),
            pltpu.VMEM(edge, F32),
            pltpu.VMEM(edge, BF16),
            pltpu.VMEM(edge, BF16),
            pltpu.VMEM((blocks, 2, 8, LANES), F32),
            pltpu.VMEM((9 * 32, LANES), F32),
            pltpu.VMEM((shards, 8, LANES), BF16),
            pltpu.VMEM((shards, 8, LANES), BF16),
            pltpu.VMEM((per, 8, LANES), F32),
            pltpu.VMEM((nx * per, 8, LANES), F32),
            pltpu.VMEM((per, 8, LANES), BF16),
            pltpu.VMEM((shards, 8, LANES), BF16),
            pltpu.VMEM((rows, chans), BF16),
            pltpu.VMEM((rows, chans), BF16),
            pltpu.SemaphoreType.DMA((5,)),
            pltpu.SemaphoreType.DMA((2,)),
            pltpu.SemaphoreType.DMA((2,)),
            pltpu.SemaphoreType.DMA((2,)),
            pltpu.SemaphoreType.DMA((2,)),
            pltpu.SemaphoreType.DMA((2,)),
            pltpu.SemaphoreType.DMA((3,)),
            pltpu.SemaphoreType.DMA((3,)),
        ],
        compiler_params=pltpu.CompilerParams(
            collective_id=0, has_side_effects=True, vmem_limit_bytes=48 * 1024 * 1024
        ),
    )(proj_a, proj_gate, cotangent, taps, norm_gain.reshape(1, -1), norm_shift.reshape(1, -1))
    a_grad, gate_grad, taps_grad, gain_grad, shift_grad = outs
    return (a_grad, gate_grad, taps_grad, gain_grad.reshape(-1), shift_grad.reshape(-1))


def solution(mesh):
    sizes = (8, 8, 4)
    torus = Mesh(mesh.devices.reshape(*sizes, mesh.shape["tp"]), (*SP, "tp"))
    return jax.shard_map(
        functools.partial(body, sizes),
        mesh=torus,
        in_specs=(P(SP, "tp"), P(SP, "tp"), P(None, "tp"), P("tp"), P("tp"), P(SP, "tp")),
        out_specs=(P(SP, "tp"), P(SP, "tp"), P(None, "tp"), P("tp"), P("tp")),
        check_vma=False,
    )
```

```python
import functools

import jax
import jax.numpy as jnp
from jax import lax
from jax.experimental import pallas as pl
from jax.experimental.pallas import tpu as pltpu
from jax.sharding import Mesh
from jax.sharding import PartitionSpec as P

SP = ("sp_0", "sp_1", "sp_2")
EPS = 1e-05
F32 = jnp.float32
BF16 = jnp.bfloat16
MESH = pl.DeviceIdType.MESH
S = 16
LANES = 128
ROWS = 256
EDGE = 30
TAPS = 31


def sigmoid(x):
    return 0.5 * jnp.tanh(0.5 * x) + 0.5


def kernel(
    sizes,
    a_hbm,
    g_hbm,
    cot_hbm,
    taps_hbm,
    gain_hbm,
    shift_hbm,
    ag_out,
    gg_out,
    tg_ref,
    gng_ref,
    shg_ref,
    a_in,
    g_in,
    cot_in,
    a_tail,
    g_tail,
    ap,
    sg,
    cotp,
    ext,
    dce,
    tapb,
    convs,
    dnorm,
    rowsum,
    rowdot,
    mean_l,
    rstd_s,
    m1_s,
    m2_s,
    stat_snd,
    stat_rcv,
    sums_snd,
    sums_rcv,
    halo_snd,
    halo_rcv,
    halo_f,
    back_f,
    back_snd,
    back_rcv,
    col,
    red,
    part,
    part_rcv,
    line_snd,
    line_rcv,
    full_snd,
    full_rcv,
    gain_ref,
    shift_ref,
    taps_in,
    in_sem,
    tp_send,
    tp_recv,
    halo_send,
    halo_recv,
    red_send,
    red_recv,
):
    nz, ny, nx = sizes
    blocks = ext.shape[0]
    chans = blocks * LANES
    plane = nz * ny
    z, y, x, core = (lax.axis_index(name) for name in (*SP, "tp"))
    sp = (z * ny + y) * nx + x
    total = plane * nx

    def place(index):
        return (index // (ny * nx), index // nx % ny, index % nx, core)

    after = place(lax.rem(sp + 1, total))
    behind = place(lax.rem(sp + total - 1, total))
    other = (z, y, x, 1 - core)
    mine = z * ny + y

    zs = [lax.rem(z + j, nz) for j in range(nz)]
    ys = [lax.rem(y + j, ny) for j in range(ny)]
    line = [(z, y, lax.rem(x + j, nx), core) for j in range(1, nx)]

    def far(n, j):
        return min(j, n - j)

    steps = sorted(
        ((j, i) for j in range(nz) for i in range(ny) if (j, i) != (0, 0)), key=lambda v: -far(nz, v[0]) - far(ny, v[1])
    )
    others = [(zs[j] * ny + ys[i], (zs[j], ys[i], x, core)) for j, i in steps]

    tail = pl.ds(ROWS - 32, 32)
    loads = [
        pltpu.make_async_copy(a_hbm.at[tail], a_tail, in_sem.at[0]),
        pltpu.make_async_copy(g_hbm.at[tail], g_tail, in_sem.at[1]),
        pltpu.make_async_copy(a_hbm, a_in, in_sem.at[2]),
        pltpu.make_async_copy(g_hbm, g_in, in_sem.at[3]),
        pltpu.make_async_copy(taps_hbm, taps_in, in_sem.at[4]),
        pltpu.make_async_copy(cot_hbm, cot_in, in_sem.at[5]),
        pltpu.make_async_copy(gain_hbm, gain_ref, in_sem.at[6]),
        pltpu.make_async_copy(shift_hbm, shift_ref, in_sem.at[7]),
    ]
    for load in loads:
        load.start()

    barrier = pltpu.get_barrier_semaphore()

    def greet(device):
        pl.semaphore_signal(barrier, inc=1, device_id=device, device_id_type=MESH)

    greet(other)
    greet(after)
    greet(behind)

    for device in line:
        greet(device)
    for _, device in others:
        greet(device)

    loads[0].wait()
    loads[1].wait()
    for c in range(blocks):
        lanes = pl.ds(c * LANES, LANES)
        halo_snd[c] = (a_tail[:, lanes].astype(F32) * sigmoid(g_tail[:, lanes].astype(F32))).astype(BF16)

    loads[4].wait()
    for c in range(blocks):
        rows = taps_in[:, c * LANES : (c + 1) * LANES].astype(F32)
        for k in range(TAPS):
            tapb[c, k] = jnp.broadcast_to(rows[k : k + 1], (S, LANES)).astype(BF16)

    at = lax.broadcasted_iota(jnp.int32, (ROWS, ROWS), 0)
    pos = lax.broadcasted_iota(jnp.int32, (ROWS, ROWS), 1)
    perm = jnp.where(pos == (at % S) * S + at // S, 1.0, 0.0).astype(BF16)
    for i in (2, 3, 5, 6, 7):
        loads[i].wait()

    def moved(v):
        return jnp.dot(perm, v, preferred_element_type=F32)

    @pl.loop(0, blocks // 2)
    def _(cc):
        wide = pl.ds(pl.multiple_of(cc * 2 * LANES, 2 * LANES), 2 * LANES)
        av = moved(a_in[:, wide])
        sv = sigmoid(moved(g_in[:, wide]))
        glu = (av * sv).astype(BF16)
        cv = moved(cot_in[:, wide])
        for h in range(2):
            lanes = slice(h * LANES, (h + 1) * LANES)
            c = cc * 2 + h
            ap[c] = av[:, lanes].astype(BF16)
            sg[c] = sv[:, lanes]
            cotp[c] = cv[:, lanes].astype(BF16)
            for r in range(S):
                ext[c, EDGE + r] = glu[r * S : (r + 1) * S, lanes]

    pl.semaphore_wait(barrier, 3 + (nx - 1) + (plane - 1))
    halo = pltpu.make_async_remote_copy(
        halo_snd, halo_rcv, halo_send.at[0], halo_recv.at[0], device_id=after, device_id_type=MESH
    )
    halo.start()
    halo.wait_recv()
    row = lax.broadcasted_iota(jnp.int32, (S, LANES), 0)

    @pl.loop(0, blocks)
    def _(c):
        halo_f[c] = jnp.where(sp > 0, halo_rcv[c].astype(F32), 0.0)

    @pl.loop(0, blocks)
    def _(c):
        for r in range(S):
            v = ext[c, EDGE + r].astype(F32)
            one = jnp.where(row == 0, halo_f[c, S + r : S + r + 1], pltpu.roll(v, 1, 0))
            ext[c, EDGE - S + r] = one.astype(BF16)
            if r >= 2:
                two = jnp.where(row == 0, halo_f[c, r : r + 1], pltpu.roll(one, 1, 0))
                ext[c, r - 2] = two.astype(BF16)

    rowsum[...] = jnp.zeros_like(rowsum)

    @pl.loop(0, blocks)
    def _(c):
        for q in range(S // 4):
            acc = [None] * 4
            for k in range(TAPS):
                tap = tapb[c, k].astype(F32)
                for i in range(4):
                    v = ext[c, q * 4 + i + k].astype(F32) * tap
                    acc[i] = v if acc[i] is None else acc[i] + v
            for i in range(4):
                convs[c, q * 4 + i] = acc[i]
                rowsum[q * 4 + i] += acc[i]

    for r in range(S):
        mean_l[r] = jnp.broadcast_to(jnp.sum(rowsum[r], axis=1, keepdims=True) / chans, (S, LANES))

    @pl.loop(0, S)
    def _(r):
        m = mean_l[r]
        acc = jnp.zeros((S, LANES), F32)
        for c in range(blocks):
            cent = convs[c, r] - m
            acc = acc + cent * cent
        rowdot[r] = acc

    lane = lax.broadcasted_iota(jnp.int32, (S, LANES), 1)
    for r in range(S):
        stat_snd[r] = jnp.where(lane == 0, mean_l[r], jnp.sum(rowdot[r], axis=1, keepdims=True))
    stat = pltpu.make_async_remote_copy(
        stat_snd, stat_rcv, tp_send.at[0], tp_recv.at[0], device_id=other, device_id_type=MESH
    )
    stat.start()
    stat.wait()
    for r in range(S):
        own_m, far_m = mean_l[r], jnp.broadcast_to(stat_rcv[r][:, 0:1], (S, LANES))
        own_q, far_q = stat_snd[r][:, 1:2], stat_rcv[r][:, 1:2]
        diff = own_m - far_m
        spread = (own_q + far_q + diff * diff * (chans / 2)) / (2 * chans)
        mean_l[r] = 0.5 * (own_m + far_m)
        rstd_s[r] = lax.rsqrt(spread + EPS)

    col[...] = jnp.zeros_like(col)

    @pl.loop(0, S)
    def _(r):
        m, rs = mean_l[r], rstd_s[r]
        acc1 = jnp.zeros((S, LANES), F32)
        acc2 = jnp.zeros((S, LANES), F32)
        for c in range(blocks):
            lanes = slice(c * LANES, (c + 1) * LANES)
            normed = (convs[c, r] - m) * rs
            gain = gain_ref[lanes].reshape(1, LANES)
            pre = normed * gain + shift_ref[lanes].reshape(1, LANES)
            sig = sigmoid(pre)
            cv = cotp[c, pl.ds(pl.multiple_of(r * S, S), S)].astype(F32)
            dpre = cv * sig * (1.0 + pre * (1.0 - sig))
            dn = dpre * gain
            convs[c, r] = normed
            dnorm[c, r] = dn
            acc1 = acc1 + dn
            acc2 = acc2 + dn * normed
            prod = dpre * normed
            col[c, 0] += prod[:8] + prod[8:]
            col[c, 1] += dpre[:8] + dpre[8:]
        rowsum[r] = acc1
        rowdot[r] = acc2

    for r in range(S):
        sums_snd[r] = jnp.where(
            lane == 0,
            jnp.sum(rowsum[r], axis=1, keepdims=True),
            jnp.sum(rowdot[r], axis=1, keepdims=True),
        )
    sums = pltpu.make_async_remote_copy(
        sums_snd, sums_rcv, tp_send.at[1], tp_recv.at[1], device_id=other, device_id_type=MESH
    )
    sums.start()
    sums.wait()
    for r in range(S):
        both = (sums_snd[r] + sums_rcv[r]) / (2 * chans)
        rs = rstd_s[r]
        m1_s[r] = rs * both[:, 0:1]
        m2_s[r] = rs * both[:, 1:2]

    @pl.loop(0, blocks)
    def _(c):
        for r in range(S):
            d = rstd_s[r] * dnorm[c, r] - m1_s[r] - convs[c, r] * m2_s[r]
            dce[c, r] = d.astype(BF16)
            back_f[c, r : r + 1] = d[0:1]
            back_f[c, S + r : S + r + 1] = d[1:2]
        back_snd[c] = back_f[c].astype(BF16)

    back = pltpu.make_async_remote_copy(
        back_snd, back_rcv, halo_send.at[1], halo_recv.at[1], device_id=behind, device_id_type=MESH
    )
    back.start()

    for extra in range(5 * blocks, part.shape[0]):
        part[extra] = jnp.zeros((8, LANES), BF16)

    @pl.loop(0, blocks)
    def _(c):
        for q in range(8):
            ks = [k for k in range(q * 4, q * 4 + 4) if k < TAPS]
            acc = [None] * len(ks)
            for r in range(S):
                d = dce[c, r].astype(F32)
                for i, k in enumerate(ks):
                    v = ext[c, k + r].astype(F32) * d
                    acc[i] = v if acc[i] is None else acc[i] + v
            for i, k in enumerate(ks):
                red[pl.ds(9 * k, 8), :] = acc[i][:8] + acc[i][8:]
        red[pl.ds(9 * TAPS, 8), :] = col[c, 0]
        for g in range(4):
            rows = red[pl.ds(72 * g, 8, stride=9), :]
            for s in range(1, 8):
                rows = rows + red[pl.ds(72 * g + s, 8, stride=9), :]
            part[5 * c + g] = rows.astype(BF16)
        part[5 * c + 4] = jnp.broadcast_to(jnp.sum(col[c, 1], axis=0, keepdims=True), (8, LANES)).astype(BF16)

    per = part.shape[0] // plane

    def shard(index):
        return pl.ds(index * per, per)

    def scatter(index, device):
        return pltpu.make_async_remote_copy(
            part.at[shard(index)],
            part_rcv.at[shard(mine)],
            red_send.at[0],
            red_recv.at[0],
            device_id=device,
            device_id_type=MESH,
        )

    for index, device in others:
        scatter(index, device).start()

    part_rcv[shard(mine)] = part[shard(mine)]

    back.wait_recv()

    @pl.loop(0, blocks)
    def _(c):
        halo_f[c] = jnp.where(sp < total - 1, back_rcv[c].astype(F32), 0.0)

    @pl.loop(0, blocks)
    def _(c):
        for r in range(S):
            v = dce[c, r].astype(F32)
            one = jnp.where(row == S - 1, halo_f[c, r : r + 1], pltpu.roll(v, S - 1, 0))
            dce[c, S + r] = one.astype(BF16)
            if r < EDGE - S:
                two = jnp.where(row == S - 1, halo_f[c, S + r : S + r + 1], pltpu.roll(one, S - 1, 0))
                dce[c, 2 * S + r] = two.astype(BF16)

    @pl.loop(0, blocks)
    def _(c):
        for q in range(S // 4):
            acc = [None] * 4
            for k in range(TAPS):
                tap = tapb[c, k].astype(F32)
                for i in range(4):
                    v = dce[c, q * 4 + i + EDGE - k].astype(F32) * tap
                    acc[i] = v if acc[i] is None else acc[i] + v
            for i in range(4):
                convs[c, q * 4 + i] = acc[i]

    @pl.loop(0, blocks // 2)
    def _(cc):
        wide = pl.ds(pl.multiple_of(cc * 2 * LANES, 2 * LANES), 2 * LANES)
        da, dg = [], []
        for h in range(2):
            c = cc * 2 + h
            grad = convs[c].reshape(ROWS, LANES)
            sv = sg[c]
            first = grad * sv
            da.append(first.astype(BF16))
            dg.append((first * ap[c].astype(F32) * (1.0 - sv)).astype(BF16))
        ag_out[:, wide] = moved(jnp.concatenate(da, axis=1)).astype(BF16)
        gg_out[:, wide] = moved(jnp.concatenate(dg, axis=1)).astype(BF16)

    def wait_all(ref, count, size, sem):
        some = ref.at[pl.ds(0, count * size)]
        pltpu.make_async_copy(some, some, sem).wait()

    wait_all(part_rcv, plane - 1, per, red_recv.at[0])
    sums8 = part_rcv[pl.ds(0, per)].astype(F32)
    for j in range(1, plane):
        sums8 = sums8 + part_rcv[pl.ds(j * per, per)].astype(F32)
    line_snd[...] = sums8
    line_rcv[pl.ds(x * per, per)] = sums8

    for device in line:
        pltpu.make_async_remote_copy(
            line_snd,
            line_rcv.at[shard(x)],
            red_send.at[1],
            red_recv.at[1],
            device_id=device,
            device_id_type=MESH,
        ).start()

    wait_all(line_rcv, nx - 1, per, red_recv.at[1])
    sums8 = line_rcv[pl.ds(0, per)]
    for j in range(1, nx):
        sums8 = sums8 + line_rcv[pl.ds(j * per, per)]
    full_snd[...] = sums8.astype(BF16)
    full_rcv[shard(mine)] = sums8.astype(BF16)

    for _, device in others:
        pltpu.make_async_remote_copy(
            full_snd,
            full_rcv.at[shard(mine)],
            red_send.at[2],
            red_recv.at[2],
            device_id=device,
            device_id_type=MESH,
        ).start()

    wait_all(full_rcv, plane - 1, per, red_recv.at[2])
    for c in range(blocks):
        lanes = slice(c * LANES, (c + 1) * LANES)
        for g in range(4):
            rows = full_rcv[5 * c + g].astype(F32)
            if g < 3:
                tg_ref[8 * g : 8 * g + 8, lanes] = rows
            else:
                tg_ref[24:TAPS, lanes] = rows[:7]
                gng_ref[lanes] = rows[7:8].reshape(LANES)
        shg_ref[lanes] = full_rcv[5 * c + 4].astype(F32)[0:1].reshape(LANES)

    halo.wait_send()
    back.wait_send()
    wait_all(part, plane - 1, per, red_send.at[0])
    wait_all(line_rcv, nx - 1, per, red_send.at[1])
    wait_all(full_rcv, plane - 1, per, red_send.at[2])


def put_out(*refs):
    count = len(refs) // 2
    sem = refs[-1]
    copies = [pltpu.make_async_copy(refs[i], refs[count + i], sem.at[i]) for i in range(count)]
    for copy in copies:
        copy.start()
    for copy in copies:
        copy.wait()


def body(sizes, proj_a, proj_gate, taps, norm_gain, norm_shift, cotangent):
    rows, chans = proj_a.shape
    blocks = chans // LANES
    nz, ny, nx = sizes
    plane = nz * ny
    per = -(-5 * blocks // plane)
    shards = per * plane
    hbm = pl.BlockSpec(memory_space=pltpu.HBM)
    vmem = pl.BlockSpec(memory_space=pltpu.VMEM)
    tile = (S, S, LANES)
    edge = (blocks, 32, LANES)
    shapes = (
        jax.ShapeDtypeStruct((rows, chans), BF16),
        jax.ShapeDtypeStruct((rows, chans), BF16),
        jax.ShapeDtypeStruct((TAPS, chans), F32),
        jax.ShapeDtypeStruct((chans,), F32),
        jax.ShapeDtypeStruct((chans,), F32),
    )
    outs = pl.pallas_call(
        functools.partial(kernel, sizes),
        out_shape=shapes,
        in_specs=[hbm] * 6,
        out_specs=(vmem,) * 5,
        scratch_shapes=[
            pltpu.VMEM((rows, chans), BF16),
            pltpu.VMEM((rows, chans), BF16),
            pltpu.VMEM((rows, chans), BF16),
            pltpu.VMEM((32, chans), BF16),
            pltpu.VMEM((32, chans), BF16),
            pltpu.VMEM((blocks, rows, LANES), BF16),
            pltpu.VMEM((blocks, rows, LANES), F32),
            pltpu.VMEM((blocks, rows, LANES), BF16),
            pltpu.VMEM((blocks, EDGE + S, S, LANES), BF16),
            pltpu.VMEM((blocks, EDGE + S, S, LANES), BF16),
            pltpu.VMEM((blocks, TAPS, S, LANES), BF16),
            pltpu.VMEM((blocks, *tile), F32),
            pltpu.VMEM((blocks, *tile), F32),
            pltpu.VMEM(tile, F32),
            pltpu.VMEM(tile, F32),
            pltpu.VMEM(tile, F32),
            pltpu.VMEM(tile, F32),
            pltpu.VMEM(tile, F32),
            pltpu.VMEM(tile, F32),
            pltpu.VMEM(tile, F32),
            pltpu.VMEM(tile, F32),
            pltpu.VMEM(tile, F32),
            pltpu.VMEM(tile, F32),
            pltpu.VMEM(edge, BF16),
            pltpu.VMEM(edge, BF16),
            pltpu.VMEM(edge, F32),
            pltpu.VMEM(edge, F32),
            pltpu.VMEM(edge, BF16),
            pltpu.VMEM(edge, BF16),
            pltpu.VMEM((blocks, 2, 8, LANES), F32),
            pltpu.VMEM((9 * 32, LANES), F32),
            pltpu.VMEM((shards, 8, LANES), BF16),
            pltpu.VMEM((shards, 8, LANES), BF16),
            pltpu.VMEM((per, 8, LANES), F32),
            pltpu.VMEM((nx * per, 8, LANES), F32),
            pltpu.VMEM((per, 8, LANES), BF16),
            pltpu.VMEM((shards, 8, LANES), BF16),
            pltpu.VMEM((chans,), F32),
            pltpu.VMEM((chans,), F32),
            pltpu.VMEM((TAPS, chans), BF16),
            pltpu.SemaphoreType.DMA((8,)),
            pltpu.SemaphoreType.DMA((2,)),
            pltpu.SemaphoreType.DMA((2,)),
            pltpu.SemaphoreType.DMA((2,)),
            pltpu.SemaphoreType.DMA((2,)),
            pltpu.SemaphoreType.DMA((3,)),
            pltpu.SemaphoreType.DMA((3,)),
        ],
        compiler_params=pltpu.CompilerParams(
            collective_id=0, has_side_effects=True, vmem_limit_bytes=50_000_000
        ),
    )(proj_a, proj_gate, cotangent, taps, norm_gain, norm_shift)
    return pl.pallas_call(
        put_out,
        out_shape=shapes,
        in_specs=[vmem] * 5,
        out_specs=(hbm,) * 5,
        scratch_shapes=[pltpu.SemaphoreType.DMA((5,))],
        compiler_params=pltpu.CompilerParams(vmem_limit_bytes=16 * 1024 * 1024),
    )(*outs)


def solution(mesh):
    sizes = (8, 8, 4)
    torus = Mesh(mesh.devices.reshape(*sizes, mesh.shape["tp"]), (*SP, "tp"))
    return jax.shard_map(
        functools.partial(body, sizes),
        mesh=torus,
        in_specs=(P(SP, "tp"), P(SP, "tp"), P(None, "tp"), P("tp"), P("tp"), P(SP, "tp")),
        out_specs=(P(SP, "tp"), P(SP, "tp"), P(None, "tp"), P("tp"), P("tp")),
        check_vma=False,
    )
```

```python
import functools

import jax
import jax.numpy as jnp
from jax import lax
from jax.experimental import pallas as pl
from jax.experimental.pallas import tpu as pltpu
from jax.sharding import Mesh
from jax.sharding import PartitionSpec as P

SP = ("sp_0", "sp_1", "sp_2")
EPS = 1e-05
F32 = jnp.float32
BF16 = jnp.bfloat16
MESH = pl.DeviceIdType.MESH
S = 16
LANES = 128
ROWS = 256
EDGE = 30
TAPS = 31


def sigmoid(x):
    return 0.5 * jnp.tanh(0.5 * x) + 0.5


def kernel(
    sizes,
    a_hbm,
    g_hbm,
    cot_hbm,
    taps_hbm,
    gain_hbm,
    shift_hbm,
    ag_hbm,
    gg_hbm,
    full_hbm,
    a_in,
    g_in,
    cot_in,
    a_tail,
    g_tail,
    ap,
    sg,
    cotp,
    ext,
    dce,
    tapb,
    convs,
    dnorm,
    rowsum,
    rowdot,
    mean_l,
    rstd_s,
    m1_s,
    m2_s,
    stat_snd,
    stat_rcv,
    sums_snd,
    sums_rcv,
    halo_snd,
    halo_rcv,
    halo_f,
    back_f,
    back_snd,
    back_rcv,
    col,
    red,
    part,
    part_rcv,
    line_snd,
    line_rcv,
    full_snd,
    full_rcv,
    ag_out,
    gg_out,
    gain_ref,
    shift_ref,
    taps_in,
    in_sem,
    tp_send,
    tp_recv,
    halo_send,
    halo_recv,
    red_send,
    red_recv,
    round_sem,
    out_sem,
):
    nz, ny, nx = sizes
    blocks = ext.shape[0]
    chans = blocks * LANES
    plane = nz * ny
    z, y, x, core = (lax.axis_index(name) for name in (*SP, "tp"))
    sp = (z * ny + y) * nx + x
    total = plane * nx

    def place(index):
        return (index // (ny * nx), index // nx % ny, index % nx, core)

    after = place(lax.rem(sp + 1, total))
    behind = place(lax.rem(sp + total - 1, total))
    other = (z, y, x, 1 - core)
    mine = z * ny + y

    zs = [lax.rem(z + j, nz) for j in range(nz)]
    ys = [lax.rem(y + j, ny) for j in range(ny)]
    line = [(z, y, lax.rem(x + j, nx), core) for j in range(1, nx)]

    def far(n, j):
        return min(j, n - j)

    steps = sorted(
        ((j, i) for j in range(nz) for i in range(ny) if (j, i) != (0, 0)), key=lambda v: -far(nz, v[0]) - far(ny, v[1])
    )
    others = [(zs[j] * ny + ys[i], (zs[j], ys[i], x, core)) for j, i in steps]

    tail = pl.ds(ROWS - 32, 32)
    loads = [
        pltpu.make_async_copy(a_hbm.at[tail], a_tail, in_sem.at[0]),
        pltpu.make_async_copy(g_hbm.at[tail], g_tail, in_sem.at[1]),
        pltpu.make_async_copy(a_hbm, a_in, in_sem.at[2]),
        pltpu.make_async_copy(g_hbm, g_in, in_sem.at[3]),
        pltpu.make_async_copy(taps_hbm, taps_in, in_sem.at[4]),
        pltpu.make_async_copy(cot_hbm, cot_in, in_sem.at[5]),
        pltpu.make_async_copy(gain_hbm, gain_ref, in_sem.at[6]),
        pltpu.make_async_copy(shift_hbm, shift_ref, in_sem.at[7]),
    ]
    for load in loads:
        load.start()

    barrier = pltpu.get_barrier_semaphore()

    def greet(device):
        pl.semaphore_signal(barrier, inc=1, device_id=device, device_id_type=MESH)

    def along_x(j):
        return (z, y, lax.rem(x + j + nx, nx), core)

    def along_y(j):
        return (z, lax.rem(y + j + ny, ny), x, core)

    def along_z(j):
        return (lax.rem(z + j + nz, nz), y, x, core)

    near = [other, after, behind] + [along(j) for along in (along_x, along_y, along_z) for j in (-1, 1)]
    for device in near:
        greet(device)

    def tell(index, along, by):
        for j in (-by, by):
            pl.semaphore_signal(round_sem.at[index], inc=1, device_id=along(j), device_id_type=MESH)

    def hear(index):
        pl.semaphore_wait(round_sem.at[index], 2)

    loads[0].wait()
    loads[1].wait()
    for c in range(blocks):
        lanes = pl.ds(c * LANES, LANES)
        halo_snd[c] = (a_tail[:, lanes].astype(F32) * sigmoid(g_tail[:, lanes].astype(F32))).astype(BF16)

    pl.semaphore_wait(barrier, len(near))
    halo = pltpu.make_async_remote_copy(
        halo_snd, halo_rcv, halo_send.at[0], halo_recv.at[0], device_id=after, device_id_type=MESH
    )
    halo.start()
    tell(0, along_x, 1)
    tell(1, along_y, 1)

    loads[4].wait()
    for c in range(blocks):
        rows = taps_in[:, c * LANES : (c + 1) * LANES].astype(F32)
        for k in range(TAPS):
            tapb[c, k] = jnp.broadcast_to(rows[k : k + 1], (S, LANES)).astype(BF16)

    at = lax.broadcasted_iota(jnp.int32, (ROWS, ROWS), 0)
    pos = lax.broadcasted_iota(jnp.int32, (ROWS, ROWS), 1)
    perm = jnp.where(pos == (at % S) * S + at // S, 1.0, 0.0).astype(BF16)
    for i in (2, 3, 5, 6, 7):
        loads[i].wait()

    def moved(v):
        return jnp.dot(perm, v, preferred_element_type=F32)

    @pl.loop(0, blocks // 2)
    def _(cc):
        wide = pl.ds(pl.multiple_of(cc * 2 * LANES, 2 * LANES), 2 * LANES)
        av = moved(a_in[:, wide])
        sv = sigmoid(moved(g_in[:, wide]))
        glu = (av * sv).astype(BF16)
        cv = moved(cot_in[:, wide])
        for h in range(2):
            lanes = slice(h * LANES, (h + 1) * LANES)
            c = cc * 2 + h
            ap[c] = av[:, lanes].astype(BF16)
            sg[c] = sv[:, lanes]
            cotp[c] = cv[:, lanes].astype(BF16)
            for r in range(S):
                ext[c, EDGE + r] = glu[r * S : (r + 1) * S, lanes]

    hear(0)
    hear(1)
    tell(2, along_y, 2)
    halo.wait_recv()
    row = lax.broadcasted_iota(jnp.int32, (S, LANES), 0)

    @pl.loop(0, blocks)
    def _(c):
        halo_f[c] = jnp.where(sp > 0, halo_rcv[c].astype(F32), 0.0)

    @pl.loop(0, blocks)
    def _(c):
        for r in range(S):
            v = ext[c, EDGE + r].astype(F32)
            one = jnp.where(row == 0, halo_f[c, S + r : S + r + 1], pltpu.roll(v, 1, 0))
            ext[c, EDGE - S + r] = one.astype(BF16)
            if r >= 2:
                two = jnp.where(row == 0, halo_f[c, r : r + 1], pltpu.roll(one, 1, 0))
                ext[c, r - 2] = two.astype(BF16)

    hear(2)
    tell(3, along_z, 1)

    rowsum[...] = jnp.zeros_like(rowsum)

    @pl.loop(0, blocks)
    def _(c):
        for q in range(S // 4):
            acc = [None] * 4
            for k in range(TAPS):
                tap = tapb[c, k].astype(F32)
                for i in range(4):
                    v = ext[c, q * 4 + i + k].astype(F32) * tap
                    acc[i] = v if acc[i] is None else acc[i] + v
            for i in range(4):
                convs[c, q * 4 + i] = acc[i]
                rowsum[q * 4 + i] += acc[i]

    for r in range(S):
        mean_l[r] = jnp.broadcast_to(jnp.sum(rowsum[r], axis=1, keepdims=True) / chans, (S, LANES))

    @pl.loop(0, S)
    def _(r):
        m = mean_l[r]
        acc = jnp.zeros((S, LANES), F32)
        for c in range(blocks):
            cent = convs[c, r] - m
            acc = acc + cent * cent
        rowdot[r] = acc

    lane = lax.broadcasted_iota(jnp.int32, (S, LANES), 1)
    for r in range(S):
        stat_snd[r] = jnp.where(lane == 0, mean_l[r], jnp.sum(rowdot[r], axis=1, keepdims=True))
    stat = pltpu.make_async_remote_copy(
        stat_snd, stat_rcv, tp_send.at[0], tp_recv.at[0], device_id=other, device_id_type=MESH
    )
    stat.start()
    hear(3)
    tell(4, along_z, 2)
    stat.wait()
    for r in range(S):
        own_m, far_m = mean_l[r], jnp.broadcast_to(stat_rcv[r][:, 0:1], (S, LANES))
        own_q, far_q = stat_snd[r][:, 1:2], stat_rcv[r][:, 1:2]
        diff = own_m - far_m
        spread = (own_q + far_q + diff * diff * (chans / 2)) / (2 * chans)
        mean_l[r] = 0.5 * (own_m + far_m)
        rstd_s[r] = lax.rsqrt(spread + EPS)

    col[...] = jnp.zeros_like(col)

    @pl.loop(0, S)
    def _(r):
        m, rs = mean_l[r], rstd_s[r]
        acc1 = jnp.zeros((S, LANES), F32)
        acc2 = jnp.zeros((S, LANES), F32)
        for c in range(blocks):
            lanes = slice(c * LANES, (c + 1) * LANES)
            normed = (convs[c, r] - m) * rs
            gain = gain_ref[lanes].reshape(1, LANES)
            pre = normed * gain + shift_ref[lanes].reshape(1, LANES)
            sig = sigmoid(pre)
            cv = cotp[c, pl.ds(pl.multiple_of(r * S, S), S)].astype(F32)
            dpre = cv * sig * (1.0 + pre * (1.0 - sig))
            dn = dpre * gain
            convs[c, r] = normed
            dnorm[c, r] = dn
            acc1 = acc1 + dn
            acc2 = acc2 + dn * normed
            prod = dpre * normed
            col[c, 0] += prod[:8] + prod[8:]
            col[c, 1] += dpre[:8] + dpre[8:]
        rowsum[r] = acc1
        rowdot[r] = acc2

    for r in range(S):
        sums_snd[r] = jnp.where(
            lane == 0,
            jnp.sum(rowsum[r], axis=1, keepdims=True),
            jnp.sum(rowdot[r], axis=1, keepdims=True),
        )
    sums = pltpu.make_async_remote_copy(
        sums_snd, sums_rcv, tp_send.at[1], tp_recv.at[1], device_id=other, device_id_type=MESH
    )
    sums.start()
    hear(4)
    tell(5, along_z, 1)
    sums.wait()
    for r in range(S):
        both = (sums_snd[r] + sums_rcv[r]) / (2 * chans)
        rs = rstd_s[r]
        m1_s[r] = rs * both[:, 0:1]
        m2_s[r] = rs * both[:, 1:2]

    @pl.loop(0, blocks)
    def _(c):
        for r in range(S):
            d = rstd_s[r] * dnorm[c, r] - m1_s[r] - convs[c, r] * m2_s[r]
            dce[c, r] = d.astype(BF16)
            back_f[c, r : r + 1] = d[0:1]
            back_f[c, S + r : S + r + 1] = d[1:2]
        back_snd[c] = back_f[c].astype(BF16)

    back = pltpu.make_async_remote_copy(
        back_snd, back_rcv, halo_send.at[1], halo_recv.at[1], device_id=behind, device_id_type=MESH
    )
    back.start()

    for extra in range(5 * blocks, part.shape[0]):
        part[extra] = jnp.zeros((8, LANES), BF16)

    @pl.loop(0, blocks)
    def _(c):
        for q in range(8):
            ks = [k for k in range(q * 4, q * 4 + 4) if k < TAPS]
            acc = [None] * len(ks)
            for r in range(S):
                d = dce[c, r].astype(F32)
                for i, k in enumerate(ks):
                    v = ext[c, k + r].astype(F32) * d
                    acc[i] = v if acc[i] is None else acc[i] + v
            for i, k in enumerate(ks):
                red[pl.ds(9 * k, 8), :] = acc[i][:8] + acc[i][8:]
        red[pl.ds(9 * TAPS, 8), :] = col[c, 0]
        for g in range(4):
            rows = red[pl.ds(72 * g, 8, stride=9), :]
            for s in range(1, 8):
                rows = rows + red[pl.ds(72 * g + s, 8, stride=9), :]
            part[5 * c + g] = rows.astype(BF16)
        part[5 * c + 4] = jnp.broadcast_to(jnp.sum(col[c, 1], axis=0, keepdims=True), (8, LANES)).astype(BF16)

    hear(5)
    per = part.shape[0] // plane

    def shard(index):
        return pl.ds(index * per, per)

    def scatter(index, device):
        return pltpu.make_async_remote_copy(
            part.at[shard(index)],
            part_rcv.at[shard(mine)],
            red_send.at[0],
            red_recv.at[0],
            device_id=device,
            device_id_type=MESH,
        )

    for index, device in others:
        scatter(index, device).start()

    part_rcv[shard(mine)] = part[shard(mine)]

    back.wait_recv()

    @pl.loop(0, blocks)
    def _(c):
        halo_f[c] = jnp.where(sp < total - 1, back_rcv[c].astype(F32), 0.0)

    @pl.loop(0, blocks)
    def _(c):
        for r in range(S):
            v = dce[c, r].astype(F32)
            one = jnp.where(row == S - 1, halo_f[c, r : r + 1], pltpu.roll(v, S - 1, 0))
            dce[c, S + r] = one.astype(BF16)
            if r < EDGE - S:
                two = jnp.where(row == S - 1, halo_f[c, S + r : S + r + 1], pltpu.roll(one, S - 1, 0))
                dce[c, 2 * S + r] = two.astype(BF16)

    @pl.loop(0, blocks)
    def _(c):
        for q in range(S // 4):
            acc = [None] * 4
            for k in range(TAPS):
                tap = tapb[c, k].astype(F32)
                for i in range(4):
                    v = dce[c, q * 4 + i + EDGE - k].astype(F32) * tap
                    acc[i] = v if acc[i] is None else acc[i] + v
            for i in range(4):
                convs[c, q * 4 + i] = acc[i]

    @pl.loop(0, blocks // 2)
    def _(cc):
        wide = pl.ds(pl.multiple_of(cc * 2 * LANES, 2 * LANES), 2 * LANES)
        da, dg = [], []
        for h in range(2):
            c = cc * 2 + h
            grad = convs[c].reshape(ROWS, LANES)
            sv = sg[c]
            first = grad * sv
            da.append(first.astype(BF16))
            dg.append((first * ap[c].astype(F32) * (1.0 - sv)).astype(BF16))
        ag_out[:, wide] = moved(jnp.concatenate(da, axis=1)).astype(BF16)
        gg_out[:, wide] = moved(jnp.concatenate(dg, axis=1)).astype(BF16)

    stores = [
        pltpu.make_async_copy(ag_out, ag_hbm, out_sem.at[0]),
        pltpu.make_async_copy(gg_out, gg_hbm, out_sem.at[1]),
    ]
    for store in stores:
        store.start()

    def wait_all(ref, count, size, sem):
        some = ref.at[pl.ds(0, count * size)]
        pltpu.make_async_copy(some, some, sem).wait()

    wait_all(part_rcv, plane - 1, per, red_recv.at[0])
    sums8 = part_rcv[pl.ds(0, per)].astype(F32)
    for j in range(1, plane):
        sums8 = sums8 + part_rcv[pl.ds(j * per, per)].astype(F32)
    line_snd[...] = sums8
    line_rcv[pl.ds(x * per, per)] = sums8

    for device in line:
        pltpu.make_async_remote_copy(
            line_snd,
            line_rcv.at[shard(x)],
            red_send.at[1],
            red_recv.at[1],
            device_id=device,
            device_id_type=MESH,
        ).start()

    wait_all(line_rcv, nx - 1, per, red_recv.at[1])
    sums8 = line_rcv[pl.ds(0, per)]
    for j in range(1, nx):
        sums8 = sums8 + line_rcv[pl.ds(j * per, per)]
    full_snd[...] = sums8.astype(BF16)
    full_rcv[shard(mine)] = sums8.astype(BF16)

    for _, device in others:
        pltpu.make_async_remote_copy(
            full_snd,
            full_rcv.at[shard(mine)],
            red_send.at[2],
            red_recv.at[2],
            device_id=device,
            device_id_type=MESH,
        ).start()

    wait_all(full_rcv, plane - 1, per, red_recv.at[2])
    whole = pltpu.make_async_copy(full_rcv, full_hbm, out_sem.at[2])
    whole.start()
    for store in stores:
        store.wait()
    halo.wait_send()
    back.wait_send()
    wait_all(part, plane - 1, per, red_send.at[0])
    wait_all(line_rcv, nx - 1, per, red_send.at[1])
    wait_all(full_rcv, plane - 1, per, red_send.at[2])
    whole.wait()


def put_out(
    pieces,
    ag_in,
    gg_in,
    full_in,
    ag_hbm,
    gg_hbm,
    tg_hbm,
    gng_hbm,
    shg_hbm,
    ag,
    gg,
    full_rcv,
    tg_ref,
    gng_ref,
    shg_ref,
    in_sem,
    out_sem,
):
    rows = ag.shape[0] // pieces
    blocks = ag.shape[1] // LANES
    first = pltpu.make_async_copy(full_in, full_rcv, in_sem.at[2 * pieces])
    first.start()
    loads, stores = [], []
    for i in range(pieces):
        part = pl.ds(i * rows, rows)
        for n, (src, held, dst) in enumerate(((ag_in, ag, ag_hbm), (gg_in, gg, gg_hbm))):
            loads.append(pltpu.make_async_copy(src.at[part], held.at[part], in_sem.at[2 * i + n]))
            stores.append(pltpu.make_async_copy(held.at[part], dst.at[part], out_sem.at[2 * i + n]))
    for load in loads:
        load.start()
    first.wait()
    for c in range(blocks):
        lanes = slice(c * LANES, (c + 1) * LANES)
        for g in range(4):
            rows = full_rcv[5 * c + g].astype(F32)
            if g < 3:
                tg_ref[8 * g : 8 * g + 8, lanes] = rows
            else:
                tg_ref[24:TAPS, lanes] = rows[:7]
                gng_ref[lanes] = rows[7:8].reshape(LANES)
        shg_ref[lanes] = full_rcv[5 * c + 4].astype(F32)[0:1].reshape(LANES)
    for n, (held, dst) in enumerate(((tg_ref, tg_hbm), (gng_ref, gng_hbm), (shg_ref, shg_hbm))):
        stores.append(pltpu.make_async_copy(held, dst, out_sem.at[2 * pieces + n]))
        stores[-1].start()
    for load, store in zip(loads, stores):
        load.wait()
        store.start()
    for store in stores:
        store.wait()


def body(sizes, proj_a, proj_gate, taps, norm_gain, norm_shift, cotangent):
    rows, chans = proj_a.shape
    blocks = chans // LANES
    nz, ny, nx = sizes
    plane = nz * ny
    per = -(-5 * blocks // plane)
    shards = per * plane
    hbm = pl.BlockSpec(memory_space=pltpu.HBM)
    tile = (S, S, LANES)
    edge = (blocks, 32, LANES)
    shapes = (
        jax.ShapeDtypeStruct((rows, chans), BF16),
        jax.ShapeDtypeStruct((rows, chans), BF16),
        jax.ShapeDtypeStruct((TAPS, chans), F32),
        jax.ShapeDtypeStruct((chans,), F32),
        jax.ShapeDtypeStruct((chans,), F32),
    )
    outs = pl.pallas_call(
        functools.partial(kernel, sizes),
        out_shape=(shapes[0], shapes[1], jax.ShapeDtypeStruct((shards, 8, LANES), BF16)),
        in_specs=[hbm] * 6,
        out_specs=(hbm,) * 3,
        scratch_shapes=[
            pltpu.VMEM((rows, chans), BF16),
            pltpu.VMEM((rows, chans), BF16),
            pltpu.VMEM((rows, chans), BF16),
            pltpu.VMEM((32, chans), BF16),
            pltpu.VMEM((32, chans), BF16),
            pltpu.VMEM((blocks, rows, LANES), BF16),
            pltpu.VMEM((blocks, rows, LANES), F32),
            pltpu.VMEM((blocks, rows, LANES), BF16),
            pltpu.VMEM((blocks, EDGE + S, S, LANES), BF16),
            pltpu.VMEM((blocks, EDGE + S, S, LANES), BF16),
            pltpu.VMEM((blocks, TAPS, S, LANES), BF16),
            pltpu.VMEM((blocks, *tile), F32),
            pltpu.VMEM((blocks, *tile), F32),
            pltpu.VMEM(tile, F32),
            pltpu.VMEM(tile, F32),
            pltpu.VMEM(tile, F32),
            pltpu.VMEM(tile, F32),
            pltpu.VMEM(tile, F32),
            pltpu.VMEM(tile, F32),
            pltpu.VMEM(tile, F32),
            pltpu.VMEM(tile, F32),
            pltpu.VMEM(tile, F32),
            pltpu.VMEM(tile, F32),
            pltpu.VMEM(edge, BF16),
            pltpu.VMEM(edge, BF16),
            pltpu.VMEM(edge, F32),
            pltpu.VMEM(edge, F32),
            pltpu.VMEM(edge, BF16),
            pltpu.VMEM(edge, BF16),
            pltpu.VMEM((blocks, 2, 8, LANES), F32),
            pltpu.VMEM((9 * 32, LANES), F32),
            pltpu.VMEM((shards, 8, LANES), BF16),
            pltpu.VMEM((shards, 8, LANES), BF16),
            pltpu.VMEM((per, 8, LANES), F32),
            pltpu.VMEM((nx * per, 8, LANES), F32),
            pltpu.VMEM((per, 8, LANES), BF16),
            pltpu.VMEM((shards, 8, LANES), BF16),
            pltpu.VMEM((rows, chans), BF16),
            pltpu.VMEM((rows, chans), BF16),
            pltpu.VMEM((chans,), F32),
            pltpu.VMEM((chans,), F32),
            pltpu.VMEM((TAPS, chans), BF16),
            pltpu.SemaphoreType.DMA((8,)),
            pltpu.SemaphoreType.DMA((2,)),
            pltpu.SemaphoreType.DMA((2,)),
            pltpu.SemaphoreType.DMA((2,)),
            pltpu.SemaphoreType.DMA((2,)),
            pltpu.SemaphoreType.DMA((3,)),
            pltpu.SemaphoreType.DMA((3,)),
            pltpu.SemaphoreType.REGULAR((6,)),
            pltpu.SemaphoreType.DMA((3,)),
        ],
        compiler_params=pltpu.CompilerParams(
            collective_id=0, has_side_effects=True, vmem_limit_bytes=64_000_000
        ),
    )(proj_a, proj_gate, cotangent, taps, norm_gain, norm_shift)
    pieces = 4
    return pl.pallas_call(
        functools.partial(put_out, pieces),
        out_shape=shapes,
        in_specs=[hbm] * 3,
        out_specs=(hbm,) * 5,
        scratch_shapes=[
            *(pltpu.VMEM(shape.shape, shape.dtype) for shape in shapes[:2]),
            pltpu.VMEM((shards, 8, LANES), BF16),
            *(pltpu.VMEM(shape.shape, shape.dtype) for shape in shapes[2:]),
            pltpu.SemaphoreType.DMA((2 * pieces + 1,)),
            pltpu.SemaphoreType.DMA((2 * pieces + 3,)),
        ],
        compiler_params=pltpu.CompilerParams(vmem_limit_bytes=64_000_000),
    )(*outs)


def solution(mesh):
    sizes = (8, 8, 4)
    torus = Mesh(mesh.devices.reshape(*sizes, mesh.shape["tp"]), (*SP, "tp"))
    return jax.shard_map(
        functools.partial(body, sizes),
        mesh=torus,
        in_specs=(P(SP, "tp"), P(SP, "tp"), P(None, "tp"), P("tp"), P("tp"), P(SP, "tp")),
        out_specs=(P(SP, "tp"), P(SP, "tp"), P(None, "tp"), P("tp"), P("tp")),
        check_vma=False,
    )
```

```python
import functools

import jax
import jax.numpy as jnp
from jax import lax
from jax.experimental import pallas as pl
from jax.experimental.pallas import tpu as pltpu
from jax.sharding import Mesh
from jax.sharding import PartitionSpec as P

SP = ("sp_0", "sp_1", "sp_2")
EPS = 1e-05
F32 = jnp.float32
BF16 = jnp.bfloat16
MESH = pl.DeviceIdType.MESH
S = 16
RUN = 14
HEAD = 32
LANES = 128
ROWS = 256
EDGE = 30
TAPS = 31


def sigmoid(x):
    return 0.5 * jnp.tanh(0.5 * x) + 0.5


def kernel(
    sizes,
    a_hbm,
    g_hbm,
    cot_hbm,
    taps_hbm,
    gain_hbm,
    shift_hbm,
    ag_hbm,
    gg_hbm,
    full_hbm,
    a_in,
    g_in,
    cot_in,
    a_tail,
    g_tail,
    sg,
    glu_n,
    work,
    dconv_n,
    ext,
    hext,
    dce,
    hdce,
    tapb,
    convs,
    dnorm,
    rowsum,
    rowdot,
    mean_l,
    rstd_s,
    m1_s,
    m2_s,
    stat_snd,
    stat_rcv,
    sums_snd,
    sums_rcv,
    halo_snd,
    halo_rcv,
    back_snd,
    back_rcv,
    col,
    red,
    part,
    part_rcv,
    line_snd,
    line_rcv,
    full_snd,
    ag_out,
    gg_out,
    gain_ref,
    shift_ref,
    taps_in,
    in_sem,
    tp_send,
    tp_recv,
    halo_send,
    halo_recv,
    red_send,
    red_recv,
    round_sem,
    out_sem,
):
    nz, ny, nx = sizes
    blocks = ext.shape[0]
    pieces = halo_send.shape[0] - 1
    group = blocks // pieces
    per = full_snd.shape[0]
    shards = part.shape[0]
    owners = shards // per
    chans = blocks * LANES
    plane = nz * ny
    z, y, x, core = (lax.axis_index(name) for name in (*SP, "tp"))
    sp = (z * ny + y) * nx + x
    total = plane * nx

    def place(index):
        return (index // (ny * nx), index // nx % ny, index % nx, core)

    after = place(lax.rem(sp + 1, total))
    behind = place(lax.rem(sp + total - 1, total))
    other = (z, y, x, 1 - core)
    mine = z * ny + y

    zs = [lax.rem(z + j, nz) for j in range(nz)]
    ys = [lax.rem(y + j, ny) for j in range(ny)]
    line = [(z, y, lax.rem(x + j, nx), core) for j in range(1, nx)]

    def far(n, j):
        return min(j, n - j)

    steps = sorted(
        ((j, i) for j in range(nz) for i in range(ny) if (j, i) != (0, 0)), key=lambda v: -far(nz, v[0]) - far(ny, v[1])
    )
    others = [(zs[j], ys[i], x, core) for j, i in steps]

    tail = pl.ds(ROWS - 32, 32)
    loads = [
        pltpu.make_async_copy(a_hbm.at[tail], a_tail, in_sem.at[0]),
        pltpu.make_async_copy(g_hbm.at[tail], g_tail, in_sem.at[1]),
        pltpu.make_async_copy(taps_hbm, taps_in, in_sem.at[2]),
        pltpu.make_async_copy(a_hbm, a_in, in_sem.at[3]),
        pltpu.make_async_copy(g_hbm, g_in, in_sem.at[4]),
        pltpu.make_async_copy(cot_hbm, cot_in, in_sem.at[5]),
        pltpu.make_async_copy(gain_hbm, gain_ref, in_sem.at[6]),
        pltpu.make_async_copy(shift_hbm, shift_ref, in_sem.at[7]),
    ]
    for load in loads:
        load.start()

    barrier = pltpu.get_barrier_semaphore()

    def greet(device):
        pl.semaphore_signal(barrier, inc=1, device_id=device, device_id_type=MESH)

    def along_x(j):
        return (z, y, lax.rem(x + j + nx, nx), core)

    sides = [along_x(-1), along_x(1)]
    lower = [z >= by for by in (1, 2)]
    upper = [z + by < nz for by in (1, 2)]
    first_sp, last_sp = sp == 0, sp == total - 1

    def around(by, signal):
        def row(j):
            return [(lax.rem(z + j * by + nz, nz), lax.rem(y + i * by + ny, ny), x, core) for i in (-1, 0, 1)]

        for device in row(0)[::2]:
            signal(device)

        @pl.when(lower[by - 1])
        def _():
            for device in row(-1):
                signal(device)

        @pl.when(upper[by - 1])
        def _():
            for device in row(1):
                signal(device)

    def count(by):
        return 2 + jnp.where(lower[by - 1], 3, 0) + jnp.where(upper[by - 1], 3, 0)

    def to_round(index):
        def signal(device):
            pl.semaphore_signal(round_sem.at[index], inc=1, device_id=device, device_id_type=MESH)

        return signal

    greet(other)
    for device in sides:
        greet(device)
    around(1, greet)

    @pl.when(jnp.logical_not(last_sp))
    def _():
        greet(after)

    @pl.when(jnp.logical_not(first_sp))
    def _():
        greet(behind)

    loads[0].wait()
    loads[1].wait()
    for c in range(blocks):
        lanes = pl.ds(c * LANES, LANES)
        halo_snd[c] = (a_tail[:, lanes].astype(F32) * sigmoid(g_tail[:, lanes].astype(F32))).astype(BF16)

    def halo(i):
        piece = pl.ds(i * group, group)
        return pltpu.make_async_remote_copy(
            halo_snd.at[piece],
            halo_rcv.at[piece],
            halo_send.at[i],
            halo_recv.at[i],
            device_id=after,
            device_id_type=MESH,
        )

    def enter():
        pl.semaphore_wait(barrier, 3 + count(1) + jnp.where(first_sp, 0, 1) + jnp.where(last_sp, 0, 1))

        @pl.when(jnp.logical_not(last_sp))
        def _():
            for i in range(pieces):
                halo(i).start()

        for device in sides:
            to_round(0)(device)
        around(1, to_round(0))

    first_x = x == 0

    @pl.when(jnp.logical_not(first_x))
    def _():
        enter()

    loads[2].wait()
    for c in range(blocks):
        rows = taps_in[:, c * LANES : (c + 1) * LANES].astype(F32)
        for k in range(TAPS):
            tapb[c, k] = jnp.broadcast_to(rows[k : k + 1], (S, LANES)).astype(BF16)

    loads[3].wait()
    loads[4].wait()

    def lanes_of(c):
        return pl.ds(pl.multiple_of(c * LANES, LANES), LANES)

    @pl.loop(0, blocks)
    def _(c):
        sv = sigmoid(g_in[:, lanes_of(c)].astype(F32))
        sg[c] = sv
        glu_n[c, HEAD:] = (a_in[:, lanes_of(c)].astype(F32) * sv).astype(BF16).astype(F32)

    @pl.loop(0, blocks)
    def _(c):
        for e in range(-EDGE, RUN):
            ext[c, e + EDGE] = glu_n[c, pl.ds(2 * HEAD + e, S, stride=RUN), :].astype(BF16)

    rowsum[...] = jnp.zeros_like(rowsum)

    def convolve(c, source, first, count, start):
        for q in range(0, count, 4):
            some = range(min(4, count - q))
            acc = [None] * len(some)
            for k in range(TAPS):
                tap = tapb[c, k].astype(F32)
                for m in some:
                    v = source[c, start(q + m, k)].astype(F32) * tap
                    acc[m] = v if acc[m] is None else acc[m] + v
            for m in some:
                yield first + q + m, acc[m]

    @pl.loop(0, blocks)
    def _(c):
        for r, v in convolve(c, ext, 0, RUN, lambda r, k: r + k):
            convs[c, r] = v
            rowsum[r] += v

    lane = lax.broadcasted_iota(jnp.int32, (S, LANES), 1)

    def exchange(snd, rcv, first, count, index):
        some = pl.ds(first, count)
        return pltpu.make_async_remote_copy(
            snd.at[some], rcv.at[some], tp_send.at[index], tp_recv.at[index], device_id=other, device_id_type=MESH
        )

    def figures(first, count, index):
        for r in range(first, first + count):
            mean_l[r] = jnp.broadcast_to(jnp.sum(rowsum[r], axis=1, keepdims=True) / chans, (S, LANES))

        @pl.loop(first, first + count)
        def _(r):
            m = mean_l[r]
            acc = jnp.zeros((S, LANES), F32)
            for c in range(blocks):
                cent = convs[c, r] - m
                acc = acc + cent * cent
            rowdot[r] = acc

        for r in range(first, first + count):
            stat_snd[r] = jnp.where(lane == 0, mean_l[r], jnp.sum(rowdot[r], axis=1, keepdims=True))
        return exchange(stat_snd, stat_rcv, first, count, index)

    def joined(first, count):
        for r in range(first, first + count):
            own_m, far_m = mean_l[r], jnp.broadcast_to(stat_rcv[r][:, 0:1], (S, LANES))
            own_q, far_q = stat_snd[r][:, 1:2], stat_rcv[r][:, 1:2]
            diff = own_m - far_m
            spread = (own_q + far_q + diff * diff * (chans / 2)) / (2 * chans)
            mean_l[r] = 0.5 * (own_m + far_m)
            rstd_s[r] = lax.rsqrt(spread + EPS)

    def swish(r, at):
        m, rs = mean_l[r], rstd_s[r]
        acc1 = jnp.zeros((S, LANES), F32)
        acc2 = jnp.zeros((S, LANES), F32)
        for c in range(blocks):
            lanes = slice(c * LANES, (c + 1) * LANES)
            normed = (convs[c, r] - m) * rs
            gain = gain_ref[lanes].reshape(1, LANES)
            half = normed * (0.5 * gain) + 0.5 * shift_ref[lanes].reshape(1, LANES)
            th = jnp.tanh(half)
            dpre = work[c, at, :] * (1.0 + th) * (1.0 + (half - half * th))
            dn = dpre * gain
            convs[c, r] = normed
            dnorm[c, r] = dn
            acc1 = acc1 + dn
            acc2 = acc2 + dn * normed
            prod = dpre * normed
            col[c, 0] += prod[:8] + prod[8:]
            col[c, 1] += dpre[:8] + dpre[8:]
        rowsum[r] = acc1
        rowdot[r] = acc2

    def sum_figures(first, count, index):
        for r in range(first, first + count):
            sums_snd[r] = jnp.where(
                lane == 0,
                jnp.sum(rowsum[r], axis=1, keepdims=True),
                jnp.sum(rowdot[r], axis=1, keepdims=True),
            )
        copy = exchange(sums_snd, sums_rcv, first, count, index)
        copy.start()
        return copy

    def sums_joined(first, count):
        for r in range(first, first + count):
            both = (sums_snd[r] + sums_rcv[r]) / (2 * chans)
            rs = rstd_s[r]
            m1_s[r] = rs * both[:, 0:1]
            m2_s[r] = rs * both[:, 1:2]

    def dconv(c, r):
        return rstd_s[r] * dnorm[c, r] - m1_s[r] - convs[c, r] * m2_s[r]

    def body_at(r):
        return pl.ds(HEAD + r, S, stride=RUN)

    def head_at(r):
        return pl.ds(r, S, stride=HEAD // S)

    stat = figures(0, RUN, 0)

    @pl.when(first_x)
    def _():
        enter()

    stat.start()
    for i in (5, 6, 7):
        loads[i].wait()

    @pl.loop(0, blocks)
    def _(c):
        work[c] = 0.5 * cot_in[:, lanes_of(c)].astype(F32)

    stat.wait()
    pl.semaphore_wait(round_sem.at[0], 2 + count(1))
    around(2, to_round(1))
    joined(0, RUN)
    col[...] = jnp.zeros_like(col)

    @pl.loop(0, RUN)
    def _(r):
        swish(r, body_at(r))

    sums = sum_figures(0, RUN, 1)

    @pl.when(first_sp)
    def _():
        glu_n[:, :HEAD] = jnp.zeros((blocks, HEAD, LANES), F32)

    @pl.when(jnp.logical_not(first_sp))
    def _():
        for i in range(pieces):
            halo(i).wait_recv()

        @pl.loop(0, blocks)
        def _(c):
            glu_n[c, :HEAD] = halo_rcv[c].astype(F32)

    @pl.loop(0, blocks)
    def _(c):
        for e in range(-EDGE, 2):
            hext[c, e + EDGE] = glu_n[c, pl.ds(HEAD + e, S, stride=2), :].astype(BF16)

    @pl.loop(0, blocks)
    def _(c):
        for r, v in convolve(c, hext, RUN, 2, lambda r, k: r + k):
            convs[c, r] = v
            rowsum[r] = jnp.where(c == 0, v, rowsum[r] + v)

    head_stat = figures(RUN, 2, 2)
    head_stat.start()
    sums.wait()
    pl.semaphore_wait(round_sem.at[1], count(2))
    to_round(2)((lax.rem(z + nz // 2, nz), y, x, core))
    sums_joined(0, RUN)

    @pl.loop(0, blocks)
    def _(c):
        for r in range(RUN):
            d = dconv(c, r)
            dce[c, r] = d.astype(BF16)
            dconv_n[c, body_at(r), :] = d

    head_stat.wait()
    joined(RUN, 2)
    for r in range(2):
        swish(RUN + r, head_at(r))
    head_sums = sum_figures(RUN, 2, 3)
    sub = lax.broadcasted_iota(jnp.int32, (8, LANES), 0)
    for q in range(shards - 4 * blocks):
        rows = jnp.zeros((8, LANES), F32)
        for c in range(8 * q, min(8 * q + 8, blocks)):
            rows = jnp.where(sub == c % 8, jnp.sum(col[c, 1], axis=0, keepdims=True), rows)
        part[4 * blocks + q] = rows.astype(BF16)
    def correlate(c, rows, store):
        for q in range(8):
            ks = [k for k in range(q * 4, q * 4 + 4) if k < TAPS]
            acc = [None] * len(ks)
            for r in rows:
                d = (dce[c, r] if r < RUN else hdce[c, r - RUN]).astype(F32)
                for m, k in enumerate(ks):
                    g = ext[c, k + r] if r < RUN else hext[c, k + r - RUN]
                    v = g.astype(F32) * d
                    acc[m] = v if acc[m] is None else acc[m] + v
            for m, k in enumerate(ks):
                store(pl.ds(9 * k, 8), acc[m][:8] + acc[m][8:])

    @pl.loop(0, blocks)
    def _(c):
        def store(at, v):
            red[c, at, :] = v

        correlate(c, range(RUN - 2), store)

    head_sums.wait()
    sums_joined(RUN, 2)

    @pl.loop(0, blocks)
    def _(c):
        for r in range(2):
            d = dconv(c, RUN + r)
            hdce[c, r] = d.astype(BF16)
            dconv_n[c, head_at(r), :] = d
        back_snd[c] = dconv_n[c, :HEAD].astype(BF16)

    back = pltpu.make_async_remote_copy(
        back_snd, back_rcv, halo_send.at[pieces], halo_recv.at[pieces], device_id=behind, device_id_type=MESH
    )

    @pl.when(jnp.logical_not(first_sp))
    def _():
        back.start()


    @pl.loop(0, blocks)
    def _(c):
        def store(at, v):
            red[c, at, :] += v

        correlate(c, range(RUN - 2, S), store)
        red[c, pl.ds(9 * TAPS, 8), :] = col[c, 0]
        for g in range(4):
            rows = red[c, pl.ds(72 * g, 8, stride=9), :]
            for s in range(1, 8):
                rows = rows + red[c, pl.ds(72 * g + s, 8, stride=9), :]
            part[4 * c + g] = rows.astype(BF16)

    pl.semaphore_wait(round_sem.at[2], 1)

    def shard(index):
        return pl.ds(index * per, per)

    for device in others:
        owner = device[0] * ny + device[1]

        @pl.when(owner < owners)
        def _():
            pltpu.make_async_remote_copy(
                part.at[shard(owner)],
                part_rcv.at[shard(mine)],
                red_send.at[0],
                red_recv.at[0],
                device_id=device,
                device_id_type=MESH,
            ).start()

    def wait_all(ref, count, sem):
        some = ref.at[pl.ds(0, count * per)]
        pltpu.make_async_copy(some, some, sem).wait()

    @pl.when(mine < owners)
    def _():
        part_rcv[shard(mine)] = part[shard(mine)]
        wait_all(part_rcv, plane - 1, red_recv.at[0])
        sums8 = part_rcv[pl.ds(0, per)].astype(F32)
        for j in range(1, plane):
            sums8 = sums8 + part_rcv[pl.ds(j * per, per)].astype(F32)
        line_snd[...] = sums8
        line_rcv[shard(x)] = sums8
        for device in line:
            pltpu.make_async_remote_copy(
                line_snd,
                line_rcv.at[shard(x)],
                red_send.at[1],
                red_recv.at[1],
                device_id=device,
                device_id_type=MESH,
            ).start()
        wait_all(line_rcv, nx - 1, red_recv.at[1])
        sums8 = line_rcv[pl.ds(0, per)]
        for j in range(1, nx):
            sums8 = sums8 + line_rcv[pl.ds(j * per, per)]
        full_snd[...] = sums8.astype(BF16)
        pltpu.make_async_copy(full_snd, full_hbm.at[shard(mine)], out_sem.at[2]).start()
        for device in others:
            pltpu.make_async_remote_copy(
                full_snd,
                full_hbm.at[shard(mine)],
                red_send.at[2],
                red_recv.at[2],
                device_id=device,
                device_id_type=MESH,
            ).start()


    @pl.when(last_sp)
    def _():
        dconv_n[:, ROWS:] = jnp.zeros((blocks, HEAD, LANES), F32)

    @pl.when(jnp.logical_not(last_sp))
    def _():
        back.wait_recv()

        @pl.loop(0, blocks)
        def _(c):
            dconv_n[c, ROWS:] = back_rcv[c].astype(F32)

    @pl.loop(0, blocks)
    def _(c):
        for e in range(RUN, RUN + EDGE):
            dce[c, e] = dconv_n[c, body_at(e), :].astype(BF16)
        for e in range(2, HEAD):
            hdce[c, e] = dconv_n[c, head_at(e), :].astype(BF16)

    @pl.loop(0, blocks)
    def _(c):
        for r, v in convolve(c, dce, 0, RUN, lambda r, k: r + EDGE - k):
            work[c, body_at(r), :] = v
        for r, v in convolve(c, hdce, 0, 2, lambda r, k: r + EDGE - k):
            work[c, head_at(r), :] = v

    @pl.loop(0, blocks)
    def _(c):
        sv = sg[c]
        first = work[c] * sv
        ag_out[:, lanes_of(c)] = first.astype(BF16)
        gg_out[:, lanes_of(c)] = (first * a_in[:, lanes_of(c)].astype(F32) * (1.0 - sv)).astype(BF16)

    stores = [
        pltpu.make_async_copy(ag_out, ag_hbm, out_sem.at[0]),
        pltpu.make_async_copy(gg_out, gg_hbm, out_sem.at[1]),
    ]
    for store in stores:
        store.start()

    @pl.when(mine < owners)
    def _():
        wait_all(full_hbm, owners - 1, red_recv.at[2])
        pltpu.make_async_copy(full_snd, full_hbm.at[shard(mine)], out_sem.at[2]).wait()

    @pl.when(mine >= owners)
    def _():
        wait_all(full_hbm, owners, red_recv.at[2])


    @pl.when(jnp.logical_not(last_sp))
    def _():
        for i in range(pieces):
            halo(i).wait_send()

    @pl.when(jnp.logical_not(first_sp))
    def _():
        back.wait_send()

    @pl.when(mine < owners)
    def _():
        wait_all(part, owners - 1, red_send.at[0])
        wait_all(line_rcv, nx - 1, red_send.at[1])
        wait_all(part_rcv, plane - 1, red_send.at[2])

    @pl.when(mine >= owners)
    def _():
        wait_all(part, owners, red_send.at[0])

    for store in stores:
        store.wait()


def put_out(
    pieces,
    ag_in,
    gg_in,
    full_in,
    ag_hbm,
    gg_hbm,
    tg_hbm,
    gng_hbm,
    shg_hbm,
    ag,
    gg,
    full_rcv,
    tg_ref,
    gng_ref,
    shg_ref,
    in_sem,
    out_sem,
):
    rows = ag.shape[0] // pieces
    blocks = ag.shape[1] // LANES
    first = pltpu.make_async_copy(full_in, full_rcv, in_sem.at[2 * pieces])
    first.start()
    loads, stores = [], []
    for i in range(pieces):
        part = pl.ds(i * rows, rows)
        for n, (src, held, dst) in enumerate(((ag_in, ag, ag_hbm), (gg_in, gg, gg_hbm))):
            loads.append(pltpu.make_async_copy(src.at[part], held.at[part], in_sem.at[2 * i + n]))
            stores.append(pltpu.make_async_copy(held.at[part], dst.at[part], out_sem.at[2 * i + n]))
    for load in loads:
        load.start()
    first.wait()
    for c in range(blocks):
        lanes = slice(c * LANES, (c + 1) * LANES)
        for g in range(4):
            rows = full_rcv[4 * c + g].astype(F32)
            if g < 3:
                tg_ref[8 * g : 8 * g + 8, lanes] = rows
            else:
                tg_ref[24:TAPS, lanes] = rows[:7]
                gng_ref[lanes] = rows[7:8].reshape(LANES)
        row = full_rcv[4 * blocks + c // 8].astype(F32)[c % 8 : c % 8 + 1]
        shg_ref[lanes] = row.reshape(LANES)
    for n, (held, dst) in enumerate(((tg_ref, tg_hbm), (gng_ref, gng_hbm), (shg_ref, shg_hbm))):
        stores.append(pltpu.make_async_copy(held, dst, out_sem.at[2 * pieces + n]))
        stores[-1].start()
    for load, store in zip(loads, stores):
        load.wait()
        store.start()
    for store in stores:
        store.wait()


def body(sizes, proj_a, proj_gate, taps, norm_gain, norm_shift, cotangent):
    rows, chans = proj_a.shape
    blocks = chans // LANES
    nz, ny, nx = sizes
    plane = nz * ny
    shards = 4 * blocks + -(-blocks // 8)
    per = -(-shards // plane)
    assert shards % per == 0
    hbm = pl.BlockSpec(memory_space=pltpu.HBM)
    tile = (S, S, LANES)
    edge = (blocks, 32, LANES)
    shapes = (
        jax.ShapeDtypeStruct((rows, chans), BF16),
        jax.ShapeDtypeStruct((rows, chans), BF16),
        jax.ShapeDtypeStruct((TAPS, chans), F32),
        jax.ShapeDtypeStruct((chans,), F32),
        jax.ShapeDtypeStruct((chans,), F32),
    )
    outs = pl.pallas_call(
        functools.partial(kernel, sizes),
        out_shape=(shapes[0], shapes[1], jax.ShapeDtypeStruct((shards, 8, LANES), BF16)),
        in_specs=[hbm] * 6,
        out_specs=(hbm,) * 3,
        scratch_shapes=[
            pltpu.VMEM((rows, chans), BF16),
            pltpu.VMEM((rows, chans), BF16),
            pltpu.VMEM((rows, chans), BF16),
            pltpu.VMEM((32, chans), BF16),
            pltpu.VMEM((32, chans), BF16),
            pltpu.VMEM((blocks, rows, LANES), F32),
            pltpu.VMEM((blocks, HEAD + rows, LANES), F32),
            pltpu.VMEM((blocks, rows, LANES), F32),
            pltpu.VMEM((blocks, rows + HEAD, LANES), F32),
            pltpu.VMEM((blocks, EDGE + RUN, S, LANES), BF16),
            pltpu.VMEM((blocks, EDGE + 2, S, LANES), BF16),
            pltpu.VMEM((blocks, EDGE + RUN, S, LANES), BF16),
            pltpu.VMEM((blocks, EDGE + 2, S, LANES), BF16),
            pltpu.VMEM((blocks, TAPS, S, LANES), BF16),
            pltpu.VMEM((blocks, *tile), F32),
            pltpu.VMEM((blocks, *tile), F32),
            pltpu.VMEM(tile, F32),
            pltpu.VMEM(tile, F32),
            pltpu.VMEM(tile, F32),
            pltpu.VMEM(tile, F32),
            pltpu.VMEM(tile, F32),
            pltpu.VMEM(tile, F32),
            pltpu.VMEM(tile, F32),
            pltpu.VMEM(tile, F32),
            pltpu.VMEM(tile, F32),
            pltpu.VMEM(tile, F32),
            pltpu.VMEM(edge, BF16),
            pltpu.VMEM(edge, BF16),
            pltpu.VMEM(edge, BF16),
            pltpu.VMEM(edge, BF16),
            pltpu.VMEM((blocks, 2, 8, LANES), F32),
            pltpu.VMEM((blocks, 9 * 32, LANES), F32),
            pltpu.VMEM((shards, 8, LANES), BF16),
            pltpu.VMEM((plane * per, 8, LANES), BF16),
            pltpu.VMEM((per, 8, LANES), F32),
            pltpu.VMEM((nx * per, 8, LANES), F32),
            pltpu.VMEM((per, 8, LANES), BF16),
            pltpu.VMEM((rows, chans), BF16),
            pltpu.VMEM((rows, chans), BF16),
            pltpu.VMEM((chans,), F32),
            pltpu.VMEM((chans,), F32),
            pltpu.VMEM((TAPS, chans), BF16),
            pltpu.SemaphoreType.DMA((8,)),
            pltpu.SemaphoreType.DMA((4,)),
            pltpu.SemaphoreType.DMA((4,)),
            pltpu.SemaphoreType.DMA((2,)),
            pltpu.SemaphoreType.DMA((2,)),
            pltpu.SemaphoreType.DMA((3,)),
            pltpu.SemaphoreType.DMA((3,)),
            pltpu.SemaphoreType.REGULAR((3,)),
            pltpu.SemaphoreType.DMA((3,)),
        ],
        compiler_params=pltpu.CompilerParams(
            collective_id=0, has_side_effects=True, vmem_limit_bytes=64_000_000
        ),
    )(proj_a, proj_gate, cotangent, taps, norm_gain, norm_shift)
    pieces = 4
    return pl.pallas_call(
        functools.partial(put_out, pieces),
        out_shape=shapes,
        in_specs=[hbm] * 3,
        out_specs=(hbm,) * 5,
        scratch_shapes=[
            *(pltpu.VMEM(shape.shape, shape.dtype) for shape in shapes[:2]),
            pltpu.VMEM((shards, 8, LANES), BF16),
            *(pltpu.VMEM(shape.shape, shape.dtype) for shape in shapes[2:]),
            pltpu.SemaphoreType.DMA((2 * pieces + 1,)),
            pltpu.SemaphoreType.DMA((2 * pieces + 3,)),
        ],
        compiler_params=pltpu.CompilerParams(vmem_limit_bytes=64_000_000),
    )(*outs)


def solution(mesh):
    sizes = (8, 8, 4)
    torus = Mesh(mesh.devices.reshape(*sizes, mesh.shape["tp"]), (*SP, "tp"))
    return jax.shard_map(
        functools.partial(body, sizes),
        mesh=torus,
        in_specs=(P(SP, "tp"), P(SP, "tp"), P(None, "tp"), P("tp"), P("tp"), P(SP, "tp")),
        out_specs=(P(SP, "tp"), P(SP, "tp"), P(None, "tp"), P("tp"), P("tp")),
        check_vma=False,
    )
```

```python
import functools

import jax
import jax.numpy as jnp
from jax import lax
from jax.experimental import pallas as pl
from jax.experimental.pallas import tpu as pltpu
from jax.sharding import Mesh
from jax.sharding import PartitionSpec as P

SP = ("sp_0", "sp_1", "sp_2")
EPS = 1e-05
F32 = jnp.float32
BF16 = jnp.bfloat16
MESH = pl.DeviceIdType.MESH
S = 16
RUN = 14
HEAD = 32
LANES = 128
ROWS = 256
EDGE = 30
TAPS = 31


def sigmoid(x):
    return 0.5 * jnp.tanh(0.5 * x) + 0.5


def kernel(
    sizes,
    a_hbm,
    g_hbm,
    cot_hbm,
    taps_hbm,
    gain_hbm,
    shift_hbm,
    ag_out,
    gg_out,
    tg_ref,
    gng_ref,
    shg_ref,
    a_in,
    g_in,
    cot_in,
    a_tail,
    g_tail,
    sg,
    glu_n,
    work,
    dconv_n,
    ext,
    hext,
    dce,
    hdce,
    tapb,
    convs,
    dnorm,
    rowsum,
    rowdot,
    mean_l,
    rstd_s,
    m1_s,
    m2_s,
    stat_snd,
    stat_rcv,
    sums_snd,
    sums_rcv,
    halo_snd,
    halo_rcv,
    back_snd,
    back_rcv,
    col,
    red,
    part,
    part_rcv,
    line_snd,
    line_rcv,
    full_snd,
    full_rcv,
    gain_ref,
    shift_ref,
    taps_in,
    in_sem,
    tp_send,
    tp_recv,
    halo_send,
    halo_recv,
    red_send,
    red_recv,
    round_sem,
):
    nz, ny, nx = sizes
    blocks = ext.shape[0]
    pieces = halo_send.shape[0] - 1
    group = blocks // pieces
    per = full_snd.shape[0]
    shards = part.shape[0]
    owners = shards // per
    chans = blocks * LANES
    plane = nz * ny
    z, y, x, core = (lax.axis_index(name) for name in (*SP, "tp"))
    sp = (z * ny + y) * nx + x
    total = plane * nx

    def place(index):
        return (index // (ny * nx), index // nx % ny, index % nx, core)

    after = place(lax.rem(sp + 1, total))
    behind = place(lax.rem(sp + total - 1, total))
    other = (z, y, x, 1 - core)
    mine = z * ny + y

    zs = [lax.rem(z + j, nz) for j in range(nz)]
    ys = [lax.rem(y + j, ny) for j in range(ny)]
    line = [(z, y, lax.rem(x + j, nx), core) for j in range(1, nx)]

    def far(n, j):
        return min(j, n - j)

    steps = sorted(
        ((j, i) for j in range(nz) for i in range(ny) if (j, i) != (0, 0)), key=lambda v: -far(nz, v[0]) - far(ny, v[1])
    )
    others = [(zs[j], ys[i], x, core) for j, i in steps]

    tail = pl.ds(ROWS - 32, 32)
    loads = [
        pltpu.make_async_copy(a_hbm.at[tail], a_tail, in_sem.at[0]),
        pltpu.make_async_copy(g_hbm.at[tail], g_tail, in_sem.at[1]),
        pltpu.make_async_copy(taps_hbm, taps_in, in_sem.at[2]),
        pltpu.make_async_copy(a_hbm, a_in, in_sem.at[3]),
        pltpu.make_async_copy(g_hbm, g_in, in_sem.at[4]),
        pltpu.make_async_copy(cot_hbm, cot_in, in_sem.at[5]),
        pltpu.make_async_copy(gain_hbm, gain_ref, in_sem.at[6]),
        pltpu.make_async_copy(shift_hbm, shift_ref, in_sem.at[7]),
    ]
    for i in (0, 1, 2, 3, 4):
        loads[i].start()

    barrier = pltpu.get_barrier_semaphore()

    def greet(device):
        pl.semaphore_signal(barrier, inc=1, device_id=device, device_id_type=MESH)

    def along_x(j):
        return (z, y, lax.rem(x + j + nx, nx), core)

    sides = [along_x(-1), along_x(1)]
    lower = [z >= by for by in (1, 2)]
    upper = [z + by < nz for by in (1, 2)]
    first_sp, last_sp = sp == 0, sp == total - 1

    def around(by, signal):
        def row(j):
            return [(lax.rem(z + j * by + nz, nz), lax.rem(y + i * by + ny, ny), x, core) for i in (-1, 0, 1)]

        for device in row(0)[::2]:
            signal(device)

        @pl.when(lower[by - 1])
        def _():
            for device in row(-1):
                signal(device)

        @pl.when(upper[by - 1])
        def _():
            for device in row(1):
                signal(device)

    def count(by):
        return 2 + jnp.where(lower[by - 1], 3, 0) + jnp.where(upper[by - 1], 3, 0)

    def to_round(index):
        def signal(device):
            pl.semaphore_signal(round_sem.at[index], inc=1, device_id=device, device_id_type=MESH)

        return signal

    greet(other)
    for device in sides:
        greet(device)
    around(1, greet)

    @pl.when(jnp.logical_not(last_sp))
    def _():
        greet(after)

    @pl.when(jnp.logical_not(first_sp))
    def _():
        greet(behind)

    loads[0].wait()
    loads[1].wait()
    for c in range(blocks):
        lanes = pl.ds(c * LANES, LANES)
        halo_snd[c] = (a_tail[:, lanes].astype(F32) * sigmoid(g_tail[:, lanes].astype(F32))).astype(BF16)

    def halo(i):
        piece = pl.ds(i * group, group)
        return pltpu.make_async_remote_copy(
            halo_snd.at[piece],
            halo_rcv.at[piece],
            halo_send.at[i],
            halo_recv.at[i],
            device_id=after,
            device_id_type=MESH,
        )

    def enter():
        pl.semaphore_wait(barrier, 3 + count(1) + jnp.where(first_sp, 0, 1) + jnp.where(last_sp, 0, 1))

        @pl.when(jnp.logical_not(last_sp))
        def _():
            for i in range(pieces):
                halo(i).start()

        for device in sides:
            to_round(0)(device)
        around(1, to_round(0))

    first_x = x == 0

    @pl.when(jnp.logical_not(first_x))
    def _():
        enter()

    loads[2].wait()
    for c in range(blocks):
        rows = taps_in[:, c * LANES : (c + 1) * LANES].astype(F32)
        for k in range(TAPS):
            tapb[c, k] = jnp.broadcast_to(rows[k : k + 1], (S, LANES)).astype(BF16)

    loads[3].wait()
    loads[4].wait()
    for i in (5, 6, 7):
        loads[i].start()

    def lanes_of(c):
        return pl.ds(pl.multiple_of(c * LANES, LANES), LANES)

    @pl.loop(0, blocks)
    def _(c):
        sv = sigmoid(g_in[:, lanes_of(c)].astype(F32))
        sg[c] = sv
        glu_n[c, HEAD:] = (a_in[:, lanes_of(c)].astype(F32) * sv).astype(BF16).astype(F32)

    @pl.loop(0, blocks)
    def _(c):
        for e in range(-EDGE, RUN):
            ext[c, e + EDGE] = glu_n[c, pl.ds(2 * HEAD + e, S, stride=RUN), :].astype(BF16)

    rowsum[...] = jnp.zeros_like(rowsum)

    def convolve(c, source, first, count, start):
        for q in range(0, count, 4):
            some = range(min(4, count - q))
            acc = [None] * len(some)
            for k in range(TAPS):
                tap = tapb[c, k].astype(F32)
                for m in some:
                    v = source[c, start(q + m, k)].astype(F32) * tap
                    acc[m] = v if acc[m] is None else acc[m] + v
            for m in some:
                yield first + q + m, acc[m]

    @pl.loop(0, blocks)
    def _(c):
        for r, v in convolve(c, ext, 0, RUN, lambda r, k: r + k):
            convs[c, r] = v
            rowsum[r] += v

    lane = lax.broadcasted_iota(jnp.int32, (S, LANES), 1)

    def exchange(snd, rcv, first, count, index):
        some = pl.ds(first, count)
        return pltpu.make_async_remote_copy(
            snd.at[some], rcv.at[some], tp_send.at[index], tp_recv.at[index], device_id=other, device_id_type=MESH
        )

    def figures(first, count, index):
        for r in range(first, first + count):
            mean_l[r] = jnp.broadcast_to(jnp.sum(rowsum[r], axis=1, keepdims=True) / chans, (S, LANES))

        @pl.loop(first, first + count)
        def _(r):
            m = mean_l[r]
            acc = jnp.zeros((S, LANES), F32)
            for c in range(blocks):
                cent = convs[c, r] - m
                acc = acc + cent * cent
            rowdot[r] = acc

        for r in range(first, first + count):
            stat_snd[r] = jnp.where(lane == 0, mean_l[r], jnp.sum(rowdot[r], axis=1, keepdims=True))
        return exchange(stat_snd, stat_rcv, first, count, index)

    def joined(first, count):
        for r in range(first, first + count):
            own_m, far_m = mean_l[r], jnp.broadcast_to(stat_rcv[r][:, 0:1], (S, LANES))
            own_q, far_q = stat_snd[r][:, 1:2], stat_rcv[r][:, 1:2]
            diff = own_m - far_m
            spread = (own_q + far_q + diff * diff * (chans / 2)) / (2 * chans)
            mean_l[r] = 0.5 * (own_m + far_m)
            rstd_s[r] = lax.rsqrt(spread + EPS)

    def swish(r, at):
        m, rs = mean_l[r], rstd_s[r]
        acc1 = jnp.zeros((S, LANES), F32)
        acc2 = jnp.zeros((S, LANES), F32)
        for c in range(blocks):
            lanes = slice(c * LANES, (c + 1) * LANES)
            normed = (convs[c, r] - m) * rs
            gain = gain_ref[lanes].reshape(1, LANES)
            half = normed * (0.5 * gain) + 0.5 * shift_ref[lanes].reshape(1, LANES)
            th = jnp.tanh(half)
            dpre = work[c, at, :] * (1.0 + th) * (1.0 + (half - half * th))
            dn = dpre * gain
            convs[c, r] = normed
            dnorm[c, r] = dn
            acc1 = acc1 + dn
            acc2 = acc2 + dn * normed
            prod = dpre * normed
            col[c, 0] += prod[:8] + prod[8:]
            col[c, 1] += dpre[:8] + dpre[8:]
        rowsum[r] = acc1
        rowdot[r] = acc2

    def sum_figures(first, count, index):
        for r in range(first, first + count):
            sums_snd[r] = jnp.where(
                lane == 0,
                jnp.sum(rowsum[r], axis=1, keepdims=True),
                jnp.sum(rowdot[r], axis=1, keepdims=True),
            )
        copy = exchange(sums_snd, sums_rcv, first, count, index)
        copy.start()
        return copy

    def sums_joined(first, count):
        for r in range(first, first + count):
            both = (sums_snd[r] + sums_rcv[r]) / (2 * chans)
            rs = rstd_s[r]
            m1_s[r] = rs * both[:, 0:1]
            m2_s[r] = rs * both[:, 1:2]

    def dconv(c, r):
        return rstd_s[r] * dnorm[c, r] - m1_s[r] - convs[c, r] * m2_s[r]

    def body_at(r):
        return pl.ds(HEAD + r, S, stride=RUN)

    def head_at(r):
        return pl.ds(r, S, stride=HEAD // S)

    stat = figures(0, RUN, 0)

    @pl.when(first_x)
    def _():
        enter()

    stat.start()
    for i in (5, 6, 7):
        loads[i].wait()

    @pl.loop(0, blocks)
    def _(c):
        work[c] = 0.5 * cot_in[:, lanes_of(c)].astype(F32)

    stat.wait()
    pl.semaphore_wait(round_sem.at[0], 2 + count(1))
    around(2, to_round(1))
    joined(0, RUN)
    col[...] = jnp.zeros_like(col)

    @pl.loop(0, RUN)
    def _(r):
        swish(r, body_at(r))

    sums = sum_figures(0, RUN, 1)

    @pl.when(first_sp)
    def _():
        glu_n[:, :HEAD] = jnp.zeros((blocks, HEAD, LANES), F32)

    @pl.when(jnp.logical_not(first_sp))
    def _():
        for i in range(pieces):
            halo(i).wait_recv()

        @pl.loop(0, blocks)
        def _(c):
            glu_n[c, :HEAD] = halo_rcv[c].astype(F32)

    @pl.loop(0, blocks)
    def _(c):
        for e in range(-EDGE, 2):
            hext[c, e + EDGE] = glu_n[c, pl.ds(HEAD + e, S, stride=2), :].astype(BF16)

    @pl.loop(0, blocks)
    def _(c):
        for r, v in convolve(c, hext, RUN, 2, lambda r, k: r + k):
            convs[c, r] = v
            rowsum[r] = jnp.where(c == 0, v, rowsum[r] + v)

    head_stat = figures(RUN, 2, 2)
    head_stat.start()
    sums.wait()
    pl.semaphore_wait(round_sem.at[1], count(2))
    to_round(2)((lax.rem(z + nz // 2, nz), y, x, core))
    sums_joined(0, RUN)

    @pl.loop(0, blocks)
    def _(c):
        for r in range(RUN):
            d = dconv(c, r)
            dce[c, r] = d.astype(BF16)
            dconv_n[c, body_at(r), :] = d

    head_stat.wait()
    joined(RUN, 2)
    for r in range(2):
        swish(RUN + r, head_at(r))
    head_sums = sum_figures(RUN, 2, 3)
    sub = lax.broadcasted_iota(jnp.int32, (8, LANES), 0)
    for q in range(shards - 4 * blocks):
        rows = jnp.zeros((8, LANES), F32)
        for c in range(8 * q, min(8 * q + 8, blocks)):
            rows = jnp.where(sub == c % 8, jnp.sum(col[c, 1], axis=0, keepdims=True), rows)
        part[4 * blocks + q] = rows.astype(BF16)
    def correlate(c, rows, store):
        for q in range(8):
            ks = [k for k in range(q * 4, q * 4 + 4) if k < TAPS]
            acc = [None] * len(ks)
            for r in rows:
                d = (dce[c, r] if r < RUN else hdce[c, r - RUN]).astype(F32)
                for m, k in enumerate(ks):
                    g = ext[c, k + r] if r < RUN else hext[c, k + r - RUN]
                    v = g.astype(F32) * d
                    acc[m] = v if acc[m] is None else acc[m] + v
            for m, k in enumerate(ks):
                store(pl.ds(9 * k, 8), acc[m][:8] + acc[m][8:])

    @pl.loop(0, blocks)
    def _(c):
        def store(at, v):
            red[c, at, :] = v

        correlate(c, range(RUN - 2), store)

    head_sums.wait()
    sums_joined(RUN, 2)

    @pl.loop(0, blocks)
    def _(c):
        for r in range(2):
            d = dconv(c, RUN + r)
            hdce[c, r] = d.astype(BF16)
            dconv_n[c, head_at(r), :] = d
        back_snd[c] = dconv_n[c, :HEAD].astype(BF16)

    back = pltpu.make_async_remote_copy(
        back_snd, back_rcv, halo_send.at[pieces], halo_recv.at[pieces], device_id=behind, device_id_type=MESH
    )

    @pl.when(jnp.logical_not(first_sp))
    def _():
        back.start()


    @pl.loop(0, blocks)
    def _(c):
        def store(at, v):
            red[c, at, :] += v

        correlate(c, range(RUN - 2, S), store)
        red[c, pl.ds(9 * TAPS, 8), :] = col[c, 0]
        for g in range(4):
            rows = red[c, pl.ds(72 * g, 8, stride=9), :]
            for s in range(1, 8):
                rows = rows + red[c, pl.ds(72 * g + s, 8, stride=9), :]
            part[4 * c + g] = rows.astype(BF16)

    pl.semaphore_wait(round_sem.at[2], 1)

    def shard(index):
        return pl.ds(index * per, per)

    for device in others:
        owner = device[0] * ny + device[1]

        @pl.when(owner < owners)
        def _():
            pltpu.make_async_remote_copy(
                part.at[shard(owner)],
                part_rcv.at[shard(mine)],
                red_send.at[0],
                red_recv.at[0],
                device_id=device,
                device_id_type=MESH,
            ).start()

    def wait_all(ref, count, sem):
        some = ref.at[pl.ds(0, count * per)]
        pltpu.make_async_copy(some, some, sem).wait()

    @pl.when(mine < owners)
    def _():
        part_rcv[shard(mine)] = part[shard(mine)]
        wait_all(part_rcv, plane - 1, red_recv.at[0])
        sums8 = part_rcv[pl.ds(0, per)].astype(F32)
        for j in range(1, plane):
            sums8 = sums8 + part_rcv[pl.ds(j * per, per)].astype(F32)
        line_snd[...] = sums8
        line_rcv[shard(x)] = sums8
        for device in line:
            pltpu.make_async_remote_copy(
                line_snd,
                line_rcv.at[shard(x)],
                red_send.at[1],
                red_recv.at[1],
                device_id=device,
                device_id_type=MESH,
            ).start()
        wait_all(line_rcv, nx - 1, red_recv.at[1])
        sums8 = line_rcv[pl.ds(0, per)]
        for j in range(1, nx):
            sums8 = sums8 + line_rcv[pl.ds(j * per, per)]
        full_snd[...] = sums8.astype(BF16)
        full_rcv[shard(mine)] = sums8.astype(BF16)
        for device in others:
            pltpu.make_async_remote_copy(
                full_snd,
                full_rcv.at[shard(mine)],
                red_send.at[2],
                red_recv.at[2],
                device_id=device,
                device_id_type=MESH,
            ).start()


    @pl.when(last_sp)
    def _():
        dconv_n[:, ROWS:] = jnp.zeros((blocks, HEAD, LANES), F32)

    @pl.when(jnp.logical_not(last_sp))
    def _():
        back.wait_recv()

        @pl.loop(0, blocks)
        def _(c):
            dconv_n[c, ROWS:] = back_rcv[c].astype(F32)

    @pl.loop(0, blocks)
    def _(c):
        for e in range(RUN, RUN + EDGE):
            dce[c, e] = dconv_n[c, body_at(e), :].astype(BF16)
        for e in range(2, HEAD):
            hdce[c, e] = dconv_n[c, head_at(e), :].astype(BF16)

    @pl.loop(0, blocks)
    def _(c):
        for r, v in convolve(c, dce, 0, RUN, lambda r, k: r + EDGE - k):
            work[c, body_at(r), :] = v
        for r, v in convolve(c, hdce, 0, 2, lambda r, k: r + EDGE - k):
            work[c, head_at(r), :] = v

    @pl.loop(0, blocks)
    def _(c):
        sv = sg[c]
        first = work[c] * sv
        ag_out[:, lanes_of(c)] = first.astype(BF16)
        gg_out[:, lanes_of(c)] = (first * a_in[:, lanes_of(c)].astype(F32) * (1.0 - sv)).astype(BF16)

    @pl.when(mine < owners)
    def _():
        wait_all(full_rcv, owners - 1, red_recv.at[2])

    @pl.when(mine >= owners)
    def _():
        wait_all(full_rcv, owners, red_recv.at[2])

    for c in range(blocks):
        lanes = slice(c * LANES, (c + 1) * LANES)
        for g in range(4):
            rows = full_rcv[4 * c + g].astype(F32)
            if g < 3:
                tg_ref[8 * g : 8 * g + 8, lanes] = rows
            else:
                tg_ref[24:TAPS, lanes] = rows[:7]
                gng_ref[lanes] = rows[7:8].reshape(LANES)
        row = full_rcv[4 * blocks + c // 8].astype(F32)[c % 8 : c % 8 + 1]
        shg_ref[lanes] = row.reshape(LANES)


    @pl.when(jnp.logical_not(last_sp))
    def _():
        for i in range(pieces):
            halo(i).wait_send()

    @pl.when(jnp.logical_not(first_sp))
    def _():
        back.wait_send()

    @pl.when(mine < owners)
    def _():
        wait_all(part, owners - 1, red_send.at[0])
        wait_all(line_rcv, nx - 1, red_send.at[1])
        wait_all(part_rcv, plane - 1, red_send.at[2])

    @pl.when(mine >= owners)
    def _():
        wait_all(part, owners, red_send.at[0])


def put_out(*refs):
    *refs, sem = refs
    count = len(refs) // 2
    copies = [pltpu.make_async_copy(refs[i], refs[count + i], sem.at[i]) for i in range(count)]
    for copy in copies:
        copy.start()
    for copy in copies:
        copy.wait()


def body(sizes, proj_a, proj_gate, taps, norm_gain, norm_shift, cotangent):
    rows, chans = proj_a.shape
    blocks = chans // LANES
    nz, ny, nx = sizes
    plane = nz * ny
    shards = 4 * blocks + -(-blocks // 8)
    per = -(-shards // plane)
    assert shards % per == 0
    hbm = pl.BlockSpec(memory_space=pltpu.HBM)
    vmem = pl.BlockSpec(memory_space=pltpu.VMEM)
    tile = (S, S, LANES)
    edge = (blocks, 32, LANES)
    shapes = (
        jax.ShapeDtypeStruct((rows, chans), BF16),
        jax.ShapeDtypeStruct((rows, chans), BF16),
        jax.ShapeDtypeStruct((TAPS, chans), F32),
        jax.ShapeDtypeStruct((chans,), F32),
        jax.ShapeDtypeStruct((chans,), F32),
    )
    outs = pl.pallas_call(
        functools.partial(kernel, sizes),
        out_shape=tuple(pltpu.VMEM(shape.shape, shape.dtype) for shape in shapes),
        in_specs=[hbm] * 6,
        out_specs=(vmem,) * 5,
        scratch_shapes=[
            pltpu.VMEM((rows, chans), BF16),
            pltpu.VMEM((rows, chans), BF16),
            pltpu.VMEM((rows, chans), BF16),
            pltpu.VMEM((32, chans), BF16),
            pltpu.VMEM((32, chans), BF16),
            pltpu.VMEM((blocks, rows, LANES), F32),
            pltpu.VMEM((blocks, HEAD + rows, LANES), F32),
            pltpu.VMEM((blocks, rows, LANES), F32),
            pltpu.VMEM((blocks, rows + HEAD, LANES), F32),
            pltpu.VMEM((blocks, EDGE + RUN, S, LANES), BF16),
            pltpu.VMEM((blocks, EDGE + 2, S, LANES), BF16),
            pltpu.VMEM((blocks, EDGE + RUN, S, LANES), BF16),
            pltpu.VMEM((blocks, EDGE + 2, S, LANES), BF16),
            pltpu.VMEM((blocks, TAPS, S, LANES), BF16),
            pltpu.VMEM((blocks, *tile), F32),
            pltpu.VMEM((blocks, *tile), F32),
            pltpu.VMEM(tile, F32),
            pltpu.VMEM(tile, F32),
            pltpu.VMEM(tile, F32),
            pltpu.VMEM(tile, F32),
            pltpu.VMEM(tile, F32),
            pltpu.VMEM(tile, F32),
            pltpu.VMEM(tile, F32),
            pltpu.VMEM(tile, F32),
            pltpu.VMEM(tile, F32),
            pltpu.VMEM(tile, F32),
            pltpu.VMEM(edge, BF16),
            pltpu.VMEM(edge, BF16),
            pltpu.VMEM(edge, BF16),
            pltpu.VMEM(edge, BF16),
            pltpu.VMEM((blocks, 2, 8, LANES), F32),
            pltpu.VMEM((blocks, 9 * 32, LANES), F32),
            pltpu.VMEM((shards, 8, LANES), BF16),
            pltpu.VMEM((plane * per, 8, LANES), BF16),
            pltpu.VMEM((per, 8, LANES), F32),
            pltpu.VMEM((nx * per, 8, LANES), F32),
            pltpu.VMEM((per, 8, LANES), BF16),
            pltpu.VMEM((shards, 8, LANES), BF16),
            pltpu.VMEM((chans,), F32),
            pltpu.VMEM((chans,), F32),
            pltpu.VMEM((TAPS, chans), BF16),
            pltpu.SemaphoreType.DMA((8,)),
            pltpu.SemaphoreType.DMA((4,)),
            pltpu.SemaphoreType.DMA((4,)),
            pltpu.SemaphoreType.DMA((2,)),
            pltpu.SemaphoreType.DMA((2,)),
            pltpu.SemaphoreType.DMA((3,)),
            pltpu.SemaphoreType.DMA((3,)),
            pltpu.SemaphoreType.REGULAR((3,)),
        ],
        compiler_params=pltpu.CompilerParams(
            collective_id=0, has_side_effects=True, vmem_limit_bytes=64_000_000
        ),
    )(proj_a, proj_gate, cotangent, taps, norm_gain, norm_shift)
    return pl.pallas_call(
        put_out,
        out_shape=shapes,
        in_specs=[vmem] * 5,
        out_specs=(hbm,) * 5,
        scratch_shapes=[pltpu.SemaphoreType.DMA((5,))],
        compiler_params=pltpu.CompilerParams(vmem_limit_bytes=16_000_000),
    )(*outs)


def solution(mesh):
    sizes = (8, 8, 4)
    torus = Mesh(mesh.devices.reshape(*sizes, mesh.shape["tp"]), (*SP, "tp"))
    return jax.shard_map(
        functools.partial(body, sizes),
        mesh=torus,
        in_specs=(P(SP, "tp"), P(SP, "tp"), P(None, "tp"), P("tp"), P("tp"), P(SP, "tp")),
        out_specs=(P(SP, "tp"), P(SP, "tp"), P(None, "tp"), P("tp"), P("tp")),
        check_vma=False,
    )
```

```python
import functools

import jax
import jax.numpy as jnp
from jax import lax
from jax.experimental import pallas as pl
from jax.experimental.pallas import tpu as pltpu
from jax.sharding import Mesh
from jax.sharding import PartitionSpec as P

SP = ("sp_0", "sp_1", "sp_2")
EPS = 1e-05
F32 = jnp.float32
BF16 = jnp.bfloat16
MESH = pl.DeviceIdType.MESH
S = 16
RUN = 14
HEAD = 32
LANES = 128
ROWS = 256
EDGE = 30
TAPS = 31


def sigmoid(x):
    return 0.5 * jnp.tanh(0.5 * x) + 0.5


def kernel(
    sizes,
    a_hbm,
    g_hbm,
    cot_hbm,
    taps_hbm,
    gain_hbm,
    shift_hbm,
    ag_out,
    gg_out,
    tg_ref,
    gng_ref,
    shg_ref,
    a_in,
    g_in,
    cot_in,
    a_tail,
    g_tail,
    sg,
    glu_n,
    work,
    dconv_n,
    ext,
    hext,
    dce,
    hdce,
    tapb,
    convs,
    dnorm,
    rowsum,
    rowdot,
    mean_l,
    rstd_s,
    m1_s,
    m2_s,
    stat_snd,
    stat_rcv,
    sums_snd,
    sums_rcv,
    halo_snd,
    halo_rcv,
    back_snd,
    back_rcv,
    col,
    red,
    part,
    part_rcv,
    line_snd,
    line_rcv,
    full_snd,
    full_rcv,
    gain_ref,
    shift_ref,
    taps_in,
    in_sem,
    tp_send,
    tp_recv,
    halo_send,
    halo_recv,
    red_send,
    red_recv,
    round_sem,
):
    nz, ny, nx = sizes
    blocks = ext.shape[0]
    pieces = halo_send.shape[0] - 1
    group = blocks // pieces
    per = full_snd.shape[0]
    shards = part.shape[0]
    owners = shards // per
    chans = blocks * LANES
    plane = nz * ny
    z, y, x, core = (lax.axis_index(name) for name in (*SP, "tp"))
    sp = (z * ny + y) * nx + x
    total = plane * nx

    def place(index):
        return (index // (ny * nx), index // nx % ny, index % nx, core)

    after = place(lax.rem(sp + 1, total))
    behind = place(lax.rem(sp + total - 1, total))
    other = (z, y, x, 1 - core)
    mine = z * ny + y

    zs = [lax.rem(z + j, nz) for j in range(nz)]
    ys = [lax.rem(y + j, ny) for j in range(ny)]
    line = [(z, y, lax.rem(x + j, nx), core) for j in range(1, nx)]

    def far(n, j):
        return min(j, n - j)

    steps = sorted(
        ((j, i) for j in range(nz) for i in range(ny) if (j, i) != (0, 0)), key=lambda v: -far(nz, v[0]) - far(ny, v[1])
    )
    others = [(zs[j], ys[i], x, core) for j, i in steps]

    tail = pl.ds(ROWS - 32, 32)
    loads = [
        pltpu.make_async_copy(a_hbm.at[tail], a_tail, in_sem.at[0]),
        pltpu.make_async_copy(g_hbm.at[tail], g_tail, in_sem.at[1]),
        pltpu.make_async_copy(taps_hbm, taps_in, in_sem.at[2]),
        *(
            pltpu.make_async_copy(src.at[:, half], dst.at[:, half], in_sem.at[3 + 2 * n + m])
            for n, half in enumerate((pl.ds(0, chans // 2), pl.ds(chans // 2, chans // 2)))
            for m, (src, dst) in enumerate(((a_hbm, a_in), (g_hbm, g_in)))
        ),
        pltpu.make_async_copy(cot_hbm, cot_in, in_sem.at[7]),
        pltpu.make_async_copy(gain_hbm, gain_ref, in_sem.at[8]),
        pltpu.make_async_copy(shift_hbm, shift_ref, in_sem.at[9]),
    ]
    for i in range(7):
        loads[i].start()

    barrier = pltpu.get_barrier_semaphore()

    def greet(device):
        pl.semaphore_signal(barrier, inc=1, device_id=device, device_id_type=MESH)

    def along_x(j):
        return (z, y, lax.rem(x + j + nx, nx), core)

    sides = [along_x(-1), along_x(1)]
    lower = [z >= by for by in (1, 2)]
    upper = [z + by < nz for by in (1, 2)]
    first_sp, last_sp = sp == 0, sp == total - 1

    def around(by, signal):
        def row(j):
            return [(lax.rem(z + j * by + nz, nz), lax.rem(y + i * by + ny, ny), x, core) for i in (-1, 0, 1)]

        for device in row(0)[::2]:
            signal(device)

        @pl.when(lower[by - 1])
        def _():
            for device in row(-1):
                signal(device)

        @pl.when(upper[by - 1])
        def _():
            for device in row(1):
                signal(device)

    def count(by):
        return 2 + jnp.where(lower[by - 1], 3, 0) + jnp.where(upper[by - 1], 3, 0)

    def to_round(index):
        def signal(device):
            pl.semaphore_signal(round_sem.at[index], inc=1, device_id=device, device_id_type=MESH)

        return signal

    greet(other)
    for device in sides:
        greet(device)
    around(1, greet)

    @pl.when(jnp.logical_not(last_sp))
    def _():
        greet(after)

    @pl.when(jnp.logical_not(first_sp))
    def _():
        greet(behind)

    loads[0].wait()
    loads[1].wait()
    for c in range(blocks):
        lanes = pl.ds(c * LANES, LANES)
        halo_snd[c] = (a_tail[:, lanes].astype(F32) * sigmoid(g_tail[:, lanes].astype(F32))).astype(BF16)

    def halo(i):
        piece = pl.ds(i * group, group)
        return pltpu.make_async_remote_copy(
            halo_snd.at[piece],
            halo_rcv.at[piece],
            halo_send.at[i],
            halo_recv.at[i],
            device_id=after,
            device_id_type=MESH,
        )

    def enter():
        pl.semaphore_wait(barrier, 3 + count(1) + jnp.where(first_sp, 0, 1) + jnp.where(last_sp, 0, 1))

        @pl.when(jnp.logical_not(last_sp))
        def _():
            for i in range(pieces):
                halo(i).start()

        for device in sides:
            to_round(0)(device)
        around(1, to_round(0))

    first_x = x == 0

    @pl.when(jnp.logical_not(first_x))
    def _():
        enter()

    loads[2].wait()
    for c in range(blocks):
        rows = taps_in[:, c * LANES : (c + 1) * LANES].astype(F32)
        for k in range(TAPS):
            tapb[c, k] = jnp.broadcast_to(rows[k : k + 1], (S, LANES)).astype(BF16)

    def lanes_of(c):
        return pl.ds(pl.multiple_of(c * LANES, LANES), LANES)

    for n in range(2):
        loads[3 + 2 * n].wait()
        loads[4 + 2 * n].wait()
        if n:
            for i in (7, 8, 9):
                loads[i].start()

        @pl.loop(n * blocks // 2, (n + 1) * blocks // 2)
        def _(c):
            sv = sigmoid(g_in[:, lanes_of(c)].astype(F32))
            sg[c] = sv
            glu_n[c, HEAD:] = (a_in[:, lanes_of(c)].astype(F32) * sv).astype(BF16).astype(F32)

    @pl.loop(0, blocks)
    def _(c):
        for e in range(-EDGE, RUN):
            ext[c, e + EDGE] = glu_n[c, pl.ds(2 * HEAD + e, S, stride=RUN), :].astype(BF16)

    rowsum[...] = jnp.zeros_like(rowsum)

    def convolve(c, source, first, count, start):
        for q in range(0, count, 4):
            some = range(min(4, count - q))
            acc = [None] * len(some)
            for k in range(TAPS):
                tap = tapb[c, k].astype(F32)
                for m in some:
                    v = source[c, start(q + m, k)].astype(F32) * tap
                    acc[m] = v if acc[m] is None else acc[m] + v
            for m in some:
                yield first + q + m, acc[m]

    @pl.loop(0, blocks)
    def _(c):
        for r, v in convolve(c, ext, 0, RUN, lambda r, k: r + k):
            convs[c, r] = v
            rowsum[r] += v

    lane = lax.broadcasted_iota(jnp.int32, (S, LANES), 1)

    def exchange(snd, rcv, index):
        return pltpu.make_async_remote_copy(
            snd, rcv, tp_send.at[index], tp_recv.at[index], device_id=other, device_id_type=MESH
        )

    def packed(pairs):
        tile = jnp.zeros((S, LANES), F32)
        for n, (one, two) in enumerate(pairs):
            tile = jnp.where(lane == 2 * n, one, jnp.where(lane == 2 * n + 1, two, tile))
        return tile

    def figures(first, count, index):
        for r in range(first, first + count):
            mean_l[r] = jnp.broadcast_to(jnp.sum(rowsum[r], axis=1, keepdims=True) * (1.0 / chans), (S, LANES))

        @pl.loop(first, first + count)
        def _(r):
            m = mean_l[r]
            acc = jnp.zeros((S, LANES), F32)
            for c in range(blocks):
                cent = convs[c, r] - m
                acc = acc + cent * cent
            rowdot[r] = acc

        stat_snd[index // 2] = packed(
            (mean_l[r], jnp.sum(rowdot[r], axis=1, keepdims=True)) for r in range(first, first + count)
        )
        return exchange(stat_snd.at[index // 2], stat_rcv.at[index // 2], index)

    def joined(first, count):
        own, far = stat_snd[first // RUN], stat_rcv[first // RUN]
        both = own + far
        diff = own - far
        for n in range(count):
            m, q = slice(2 * n, 2 * n + 1), slice(2 * n + 1, 2 * n + 2)
            spread = (both[:, q] + diff[:, m] * diff[:, m] * (chans / 2)) * (0.5 / chans)
            mean_l[first + n] = jnp.broadcast_to(0.5 * both[:, m], (S, LANES))
            rstd_s[first + n] = jnp.broadcast_to(lax.rsqrt(spread + EPS), (S, LANES))

    def swish(r, at):
        m, rs = mean_l[r], rstd_s[r]
        acc1 = jnp.zeros((S, LANES), F32)
        acc2 = jnp.zeros((S, LANES), F32)
        for c in range(blocks):
            lanes = slice(c * LANES, (c + 1) * LANES)
            normed = (convs[c, r] - m) * rs
            gain = gain_ref[lanes].reshape(1, LANES)
            half = normed * (0.5 * gain) + 0.5 * shift_ref[lanes].reshape(1, LANES)
            th = jnp.tanh(half)
            dpre = work[c, at, :] * (1.0 + th) * (1.0 + (half - half * th))
            dn = dpre * gain
            convs[c, r] = normed
            dnorm[c, r] = dn
            acc1 = acc1 + dn
            acc2 = acc2 + dn * normed
            prod = dpre * normed
            col[c, 0] += prod[:8] + prod[8:]
            col[c, 1] += dpre[:8] + dpre[8:]
        rowsum[r] = acc1
        rowdot[r] = acc2

    def sum_figures(first, count, index):
        sums_snd[index // 2] = packed(
            (jnp.sum(rowsum[r], axis=1, keepdims=True), jnp.sum(rowdot[r], axis=1, keepdims=True))
            for r in range(first, first + count)
        )
        copy = exchange(sums_snd.at[index // 2], sums_rcv.at[index // 2], index)
        copy.start()
        return copy

    def sums_joined(first, count):
        both = (sums_snd[first // RUN] + sums_rcv[first // RUN]) * (0.5 / chans)
        for n in range(count):
            rs = rstd_s[first + n]
            m1_s[first + n] = rs * both[:, 2 * n : 2 * n + 1]
            m2_s[first + n] = rs * both[:, 2 * n + 1 : 2 * n + 2]

    def dconv(c, r):
        return rstd_s[r] * dnorm[c, r] - m1_s[r] - convs[c, r] * m2_s[r]

    def body_at(r):
        return pl.ds(HEAD + r, S, stride=RUN)

    def head_at(r):
        return pl.ds(r, S, stride=HEAD // S)

    stat = figures(0, RUN, 0)

    @pl.when(first_x)
    def _():
        enter()

    stat.start()
    pl.semaphore_wait(round_sem.at[0], 2 + count(1))
    around(2, to_round(1))
    for i in (7, 8, 9):
        loads[i].wait()

    @pl.loop(0, blocks)
    def _(c):
        work[c] = 0.5 * cot_in[:, lanes_of(c)].astype(F32)

    stat.wait()
    joined(0, RUN)
    col[...] = jnp.zeros_like(col)

    @pl.loop(0, RUN)
    def _(r):
        swish(r, body_at(r))

    sums = sum_figures(0, RUN, 1)

    @pl.when(first_sp)
    def _():
        glu_n[:, :HEAD] = jnp.zeros((blocks, HEAD, LANES), F32)

    @pl.when(jnp.logical_not(first_sp))
    def _():
        for i in range(pieces):
            halo(i).wait_recv()

        @pl.loop(0, blocks)
        def _(c):
            glu_n[c, :HEAD] = halo_rcv[c].astype(F32)

    @pl.loop(0, blocks)
    def _(c):
        for e in range(-EDGE, 2):
            hext[c, e + EDGE] = glu_n[c, pl.ds(HEAD + e, S, stride=2), :].astype(BF16)

    @pl.loop(0, blocks)
    def _(c):
        for r, v in convolve(c, hext, RUN, 2, lambda r, k: r + k):
            convs[c, r] = v
            rowsum[r] = jnp.where(c == 0, v, rowsum[r] + v)

    head_stat = figures(RUN, 2, 2)
    head_stat.start()
    sums.wait()
    pl.semaphore_wait(round_sem.at[1], count(2))
    to_round(2)((lax.rem(z + nz // 2, nz), y, x, core))
    sums_joined(0, RUN)

    @pl.loop(0, blocks)
    def _(c):
        for r in range(RUN):
            d = dconv(c, r)
            dce[c, r] = d.astype(BF16)
            dconv_n[c, body_at(r), :] = d

    head_stat.wait()
    joined(RUN, 2)
    for r in range(2):
        swish(RUN + r, head_at(r))
    head_sums = sum_figures(RUN, 2, 3)
    sub = lax.broadcasted_iota(jnp.int32, (8, LANES), 0)
    for q in range(shards - 4 * blocks):
        rows = jnp.zeros((8, LANES), F32)
        for c in range(8 * q, min(8 * q + 8, blocks)):
            rows = jnp.where(sub == c % 8, jnp.sum(col[c, 1], axis=0, keepdims=True), rows)
        part[4 * blocks + q] = rows.astype(BF16)
    def correlate(c, rows, store):
        for q in range(8):
            ks = [k for k in range(q * 4, q * 4 + 4) if k < TAPS]
            acc = [None] * len(ks)
            for r in rows:
                d = (dce[c, r] if r < RUN else hdce[c, r - RUN]).astype(F32)
                for m, k in enumerate(ks):
                    g = ext[c, k + r] if r < RUN else hext[c, k + r - RUN]
                    v = g.astype(F32) * d
                    acc[m] = v if acc[m] is None else acc[m] + v
            for m, k in enumerate(ks):
                store(pl.ds(9 * k, 8), acc[m][:8] + acc[m][8:])

    @pl.loop(0, blocks)
    def _(c):
        def store(at, v):
            red[c, at, :] = v

        correlate(c, range(RUN - 2), store)

    head_sums.wait()
    sums_joined(RUN, 2)

    @pl.loop(0, blocks)
    def _(c):
        for r in range(2):
            d = dconv(c, RUN + r)
            hdce[c, r] = d.astype(BF16)
            dconv_n[c, head_at(r), :] = d
        back_snd[c] = dconv_n[c, :HEAD].astype(BF16)

    back = pltpu.make_async_remote_copy(
        back_snd, back_rcv, halo_send.at[pieces], halo_recv.at[pieces], device_id=behind, device_id_type=MESH
    )

    @pl.when(jnp.logical_not(first_sp))
    def _():
        back.start()


    @pl.loop(0, blocks)
    def _(c):
        def store(at, v):
            red[c, at, :] += v

        correlate(c, range(RUN - 2, S), store)
        red[c, pl.ds(9 * TAPS, 8), :] = col[c, 0]
        for g in range(4):
            rows = red[c, pl.ds(72 * g, 8, stride=9), :]
            for s in range(1, 8):
                rows = rows + red[c, pl.ds(72 * g + s, 8, stride=9), :]
            part[4 * c + g] = rows.astype(BF16)

    pl.semaphore_wait(round_sem.at[2], 1)

    def shard(index):
        return pl.ds(index * per, per)

    for device in others:
        owner = device[0] * ny + device[1]

        @pl.when(owner < owners)
        def _():
            pltpu.make_async_remote_copy(
                part.at[shard(owner)],
                part_rcv.at[shard(mine)],
                red_send.at[0],
                red_recv.at[0],
                device_id=device,
                device_id_type=MESH,
            ).start()

    def wait_all(ref, count, sem):
        some = ref.at[pl.ds(0, count * per)]
        pltpu.make_async_copy(some, some, sem).wait()

    @pl.when(mine < owners)
    def _():
        part_rcv[shard(mine)] = part[shard(mine)]
        wait_all(part_rcv, plane - 1, red_recv.at[0])
        sums8 = part_rcv[pl.ds(0, per)].astype(F32)
        for j in range(1, plane):
            sums8 = sums8 + part_rcv[pl.ds(j * per, per)].astype(F32)
        line_snd[...] = sums8
        line_rcv[shard(x)] = sums8
        for device in line:
            pltpu.make_async_remote_copy(
                line_snd,
                line_rcv.at[shard(x)],
                red_send.at[1],
                red_recv.at[1],
                device_id=device,
                device_id_type=MESH,
            ).start()
        wait_all(line_rcv, nx - 1, red_recv.at[1])
        sums8 = line_rcv[pl.ds(0, per)]
        for j in range(1, nx):
            sums8 = sums8 + line_rcv[pl.ds(j * per, per)]
        full_snd[...] = sums8.astype(BF16)
        full_rcv[shard(mine)] = sums8.astype(BF16)
        for device in others:
            pltpu.make_async_remote_copy(
                full_snd,
                full_rcv.at[shard(mine)],
                red_send.at[2],
                red_recv.at[2],
                device_id=device,
                device_id_type=MESH,
            ).start()


    @pl.when(last_sp)
    def _():
        dconv_n[:, ROWS:] = jnp.zeros((blocks, HEAD, LANES), F32)

    @pl.when(jnp.logical_not(last_sp))
    def _():
        back.wait_recv()

        @pl.loop(0, blocks)
        def _(c):
            dconv_n[c, ROWS:] = back_rcv[c].astype(F32)

    @pl.loop(0, blocks)
    def _(c):
        for e in range(RUN, RUN + EDGE):
            dce[c, e] = dconv_n[c, body_at(e), :].astype(BF16)
        for e in range(2, HEAD):
            hdce[c, e] = dconv_n[c, head_at(e), :].astype(BF16)

    @pl.loop(0, blocks)
    def _(c):
        for r, v in convolve(c, dce, 0, RUN, lambda r, k: r + EDGE - k):
            work[c, body_at(r), :] = v
        for r, v in convolve(c, hdce, 0, 2, lambda r, k: r + EDGE - k):
            work[c, head_at(r), :] = v

    @pl.loop(0, blocks)
    def _(c):
        sv = sg[c]
        first = work[c] * sv
        ag_out[:, lanes_of(c)] = first.astype(BF16)
        gg_out[:, lanes_of(c)] = (first * a_in[:, lanes_of(c)].astype(F32) * (1.0 - sv)).astype(BF16)

    @pl.when(mine < owners)
    def _():
        wait_all(full_rcv, owners - 1, red_recv.at[2])

    @pl.when(mine >= owners)
    def _():
        wait_all(full_rcv, owners, red_recv.at[2])

    for c in range(blocks):
        lanes = slice(c * LANES, (c + 1) * LANES)
        for g in range(4):
            rows = full_rcv[4 * c + g].astype(F32)
            if g < 3:
                tg_ref[8 * g : 8 * g + 8, lanes] = rows
            else:
                tg_ref[24:TAPS, lanes] = rows[:7]
                gng_ref[lanes] = rows[7:8].reshape(LANES)
        row = full_rcv[4 * blocks + c // 8].astype(F32)[c % 8 : c % 8 + 1]
        shg_ref[lanes] = row.reshape(LANES)


    @pl.when(jnp.logical_not(last_sp))
    def _():
        for i in range(pieces):
            halo(i).wait_send()

    @pl.when(jnp.logical_not(first_sp))
    def _():
        back.wait_send()

    @pl.when(mine < owners)
    def _():
        wait_all(part, owners - 1, red_send.at[0])
        wait_all(line_rcv, nx - 1, red_send.at[1])
        wait_all(part_rcv, plane - 1, red_send.at[2])

    @pl.when(mine >= owners)
    def _():
        wait_all(part, owners, red_send.at[0])


def put_out(*refs):
    *refs, sem = refs
    count = len(refs) // 2
    copies = [pltpu.make_async_copy(refs[i], refs[count + i], sem.at[i]) for i in range(count)]
    for copy in copies:
        copy.start()
    for copy in copies:
        copy.wait()


def body(sizes, proj_a, proj_gate, taps, norm_gain, norm_shift, cotangent):
    rows, chans = proj_a.shape
    blocks = chans // LANES
    nz, ny, nx = sizes
    plane = nz * ny
    shards = 4 * blocks + -(-blocks // 8)
    per = -(-shards // plane)
    assert shards % per == 0
    hbm = pl.BlockSpec(memory_space=pltpu.HBM)
    vmem = pl.BlockSpec(memory_space=pltpu.VMEM)
    tile = (S, S, LANES)
    edge = (blocks, 32, LANES)
    shapes = (
        jax.ShapeDtypeStruct((rows, chans), BF16),
        jax.ShapeDtypeStruct((rows, chans), BF16),
        jax.ShapeDtypeStruct((TAPS, chans), F32),
        jax.ShapeDtypeStruct((chans,), F32),
        jax.ShapeDtypeStruct((chans,), F32),
    )
    outs = pl.pallas_call(
        functools.partial(kernel, sizes),
        out_shape=tuple(pltpu.VMEM(shape.shape, shape.dtype) for shape in shapes),
        in_specs=[hbm] * 6,
        out_specs=(vmem,) * 5,
        scratch_shapes=[
            pltpu.VMEM((rows, chans), BF16),
            pltpu.VMEM((rows, chans), BF16),
            pltpu.VMEM((rows, chans), BF16),
            pltpu.VMEM((32, chans), BF16),
            pltpu.VMEM((32, chans), BF16),
            pltpu.VMEM((blocks, rows, LANES), F32),
            pltpu.VMEM((blocks, HEAD + rows, LANES), F32),
            pltpu.VMEM((blocks, rows, LANES), F32),
            pltpu.VMEM((blocks, rows + HEAD, LANES), F32),
            pltpu.VMEM((blocks, EDGE + RUN, S, LANES), BF16),
            pltpu.VMEM((blocks, EDGE + 2, S, LANES), BF16),
            pltpu.VMEM((blocks, EDGE + RUN, S, LANES), BF16),
            pltpu.VMEM((blocks, EDGE + 2, S, LANES), BF16),
            pltpu.VMEM((blocks, TAPS, S, LANES), BF16),
            pltpu.VMEM((blocks, *tile), F32),
            pltpu.VMEM((blocks, *tile), F32),
            pltpu.VMEM(tile, F32),
            pltpu.VMEM(tile, F32),
            pltpu.VMEM(tile, F32),
            pltpu.VMEM(tile, F32),
            pltpu.VMEM(tile, F32),
            pltpu.VMEM(tile, F32),
            pltpu.VMEM((2, S, LANES), F32),
            pltpu.VMEM((2, S, LANES), F32),
            pltpu.VMEM((2, S, LANES), F32),
            pltpu.VMEM((2, S, LANES), F32),
            pltpu.VMEM(edge, BF16),
            pltpu.VMEM(edge, BF16),
            pltpu.VMEM(edge, BF16),
            pltpu.VMEM(edge, BF16),
            pltpu.VMEM((blocks, 2, 8, LANES), F32),
            pltpu.VMEM((blocks, 9 * 32, LANES), F32),
            pltpu.VMEM((shards, 8, LANES), BF16),
            pltpu.VMEM((plane * per, 8, LANES), BF16),
            pltpu.VMEM((per, 8, LANES), F32),
            pltpu.VMEM((nx * per, 8, LANES), F32),
            pltpu.VMEM((per, 8, LANES), BF16),
            pltpu.VMEM((shards, 8, LANES), BF16),
            pltpu.VMEM((chans,), F32),
            pltpu.VMEM((chans,), F32),
            pltpu.VMEM((TAPS, chans), BF16),
            pltpu.SemaphoreType.DMA((10,)),
            pltpu.SemaphoreType.DMA((4,)),
            pltpu.SemaphoreType.DMA((4,)),
            pltpu.SemaphoreType.DMA((2,)),
            pltpu.SemaphoreType.DMA((2,)),
            pltpu.SemaphoreType.DMA((3,)),
            pltpu.SemaphoreType.DMA((3,)),
            pltpu.SemaphoreType.REGULAR((3,)),
        ],
        compiler_params=pltpu.CompilerParams(
            collective_id=0, has_side_effects=True, vmem_limit_bytes=64_000_000
        ),
    )(proj_a, proj_gate, cotangent, taps, norm_gain, norm_shift)
    return pl.pallas_call(
        put_out,
        out_shape=shapes,
        in_specs=[vmem] * 5,
        out_specs=(hbm,) * 5,
        scratch_shapes=[pltpu.SemaphoreType.DMA((5,))],
        compiler_params=pltpu.CompilerParams(vmem_limit_bytes=16_000_000),
    )(*outs)


def solution(mesh):
    sizes = (8, 8, 4)
    torus = Mesh(mesh.devices.reshape(*sizes, mesh.shape["tp"]), (*SP, "tp"))
    return jax.shard_map(
        functools.partial(body, sizes),
        mesh=torus,
        in_specs=(P(SP, "tp"), P(SP, "tp"), P(None, "tp"), P("tp"), P("tp"), P(SP, "tp")),
        out_specs=(P(SP, "tp"), P(SP, "tp"), P(None, "tp"), P("tp"), P("tp")),
        check_vma=False,
    )
```

```python
import functools

import jax
import jax.numpy as jnp
from jax import lax
from jax.experimental import pallas as pl
from jax.experimental.pallas import tpu as pltpu
from jax.sharding import Mesh
from jax.sharding import PartitionSpec as P

SP = ("sp_0", "sp_1", "sp_2")
EPS = 1e-05
F32 = jnp.float32
BF16 = jnp.bfloat16
MESH = pl.DeviceIdType.MESH
S = 16
RUN = 14
HEAD = 32
LANES = 128
ROWS = 256
EDGE = 30
TAPS = 31


def sigmoid(x):
    return 0.5 * jnp.tanh(0.5 * x) + 0.5


def kernel(
    sizes,
    a_hbm,
    g_hbm,
    cot_hbm,
    taps_hbm,
    gain_hbm,
    shift_hbm,
    ag_out,
    gg_out,
    tg_ref,
    gng_ref,
    shg_ref,
    a_in,
    g_in,
    cot_in,
    a_tail,
    g_tail,
    sg,
    glu_n,
    work,
    dconv_n,
    ext,
    hext,
    dce,
    hdce,
    tapb,
    convs,
    dnorm,
    rowsum,
    rowdot,
    mean_l,
    rstd_s,
    m1_s,
    m2_s,
    stat_snd,
    stat_rcv,
    sums_snd,
    sums_rcv,
    halo_snd,
    halo_rcv,
    back_snd,
    back_rcv,
    col,
    red,
    part,
    part_rcv,
    line_snd,
    line_rcv,
    full_snd,
    full_rcv,
    gain_ref,
    shift_ref,
    taps_in,
    in_sem,
    tp_send,
    tp_recv,
    halo_send,
    halo_recv,
    red_send,
    red_recv,
    round_sem,
):
    nz, ny, nx = sizes
    blocks = ext.shape[0]
    pieces = halo_send.shape[0] - 1
    group = blocks // pieces
    per = full_snd.shape[0]
    shards = part.shape[0]
    owners = shards // per
    chans = blocks * LANES
    plane = nz * ny
    z, y, x, core = (lax.axis_index(name) for name in (*SP, "tp"))
    sp = (z * ny + y) * nx + x
    total = plane * nx

    def place(index):
        return (index // (ny * nx), index // nx % ny, index % nx, core)

    after = place(lax.rem(sp + 1, total))
    behind = place(lax.rem(sp + total - 1, total))
    other = (z, y, x, 1 - core)
    mine = z * ny + y

    zs = [lax.rem(z + j, nz) for j in range(nz)]
    ys = [lax.rem(y + j, ny) for j in range(ny)]
    line = [(z, y, lax.rem(x + j, nx), core) for j in range(1, nx)]

    def far(n, j):
        return min(j, n - j)

    steps = sorted(
        ((j, i) for j in range(nz) for i in range(ny) if (j, i) != (0, 0)), key=lambda v: -far(nz, v[0]) - far(ny, v[1])
    )
    others = [(zs[j], ys[i], x, core) for j, i in steps]

    tail = pl.ds(ROWS - 32, 32)
    loads = [
        pltpu.make_async_copy(a_hbm.at[tail], a_tail, in_sem.at[0]),
        pltpu.make_async_copy(g_hbm.at[tail], g_tail, in_sem.at[1]),
        pltpu.make_async_copy(taps_hbm, taps_in, in_sem.at[2]),
        *(
            pltpu.make_async_copy(src.at[:, half], dst.at[:, half], in_sem.at[3 + 2 * n + m])
            for n, half in enumerate((pl.ds(0, chans // 2), pl.ds(chans // 2, chans // 2)))
            for m, (src, dst) in enumerate(((a_hbm, a_in), (g_hbm, g_in)))
        ),
        pltpu.make_async_copy(cot_hbm, cot_in, in_sem.at[7]),
        pltpu.make_async_copy(gain_hbm, gain_ref, in_sem.at[8]),
        pltpu.make_async_copy(shift_hbm, shift_ref, in_sem.at[9]),
    ]
    for i in range(7):
        loads[i].start()

    barrier = pltpu.get_barrier_semaphore()

    def greet(device):
        pl.semaphore_signal(barrier, inc=1, device_id=device, device_id_type=MESH)

    def along_x(j):
        return (z, y, lax.rem(x + j + nx, nx), core)

    sides = [along_x(-1), along_x(1)]
    lower = [z >= by for by in (1, 2)]
    upper = [z + by < nz for by in (1, 2)]
    first_sp, last_sp = sp == 0, sp == total - 1

    def around(by, signal):
        def row(j):
            return [(lax.rem(z + j * by + nz, nz), lax.rem(y + i * by + ny, ny), x, core) for i in (-1, 0, 1)]

        for device in row(0)[::2]:
            signal(device)

        @pl.when(lower[by - 1])
        def _():
            for device in row(-1):
                signal(device)

        @pl.when(upper[by - 1])
        def _():
            for device in row(1):
                signal(device)

    def count(by):
        return 2 + jnp.where(lower[by - 1], 3, 0) + jnp.where(upper[by - 1], 3, 0)

    def to_round(index):
        def signal(device):
            pl.semaphore_signal(round_sem.at[index], inc=1, device_id=device, device_id_type=MESH)

        return signal

    greet(other)
    for device in sides:
        greet(device)
    around(1, greet)

    @pl.when(jnp.logical_not(last_sp))
    def _():
        greet(after)

    @pl.when(jnp.logical_not(first_sp))
    def _():
        greet(behind)

    loads[0].wait()
    loads[1].wait()
    for c in range(blocks):
        lanes = pl.ds(c * LANES, LANES)
        halo_snd[c] = (a_tail[:, lanes].astype(F32) * sigmoid(g_tail[:, lanes].astype(F32))).astype(BF16)

    def halo(i):
        piece = pl.ds(i * group, group)
        return pltpu.make_async_remote_copy(
            halo_snd.at[piece],
            halo_rcv.at[piece],
            halo_send.at[i],
            halo_recv.at[i],
            device_id=after,
            device_id_type=MESH,
        )

    def enter():
        pl.semaphore_wait(barrier, 3 + count(1) + jnp.where(first_sp, 0, 1) + jnp.where(last_sp, 0, 1))

        @pl.when(jnp.logical_not(last_sp))
        def _():
            for i in range(pieces):
                halo(i).start()

        for device in sides:
            to_round(0)(device)
        around(1, to_round(0))

    first_x = x == 0

    @pl.when(jnp.logical_not(first_x))
    def _():
        enter()

    loads[2].wait()
    for c in range(blocks):
        rows = taps_in[:, c * LANES : (c + 1) * LANES].astype(F32)
        for k in range(TAPS):
            tapb[c, k] = jnp.broadcast_to(rows[k : k + 1], (S, LANES)).astype(BF16)

    def lanes_of(c):
        return pl.ds(pl.multiple_of(c * LANES, LANES), LANES)

    for n in range(2):
        loads[3 + 2 * n].wait()
        loads[4 + 2 * n].wait()
        if n:
            for i in (7, 8, 9):
                loads[i].start()

        @pl.loop(n * blocks // 2, (n + 1) * blocks // 2)
        def _(c):
            sv = sigmoid(g_in[:, lanes_of(c)].astype(F32))
            sg[c] = sv
            glu_n[c, HEAD:] = (a_in[:, lanes_of(c)].astype(F32) * sv).astype(BF16).astype(F32)

    @pl.loop(0, blocks)
    def _(c):
        for e in range(-EDGE, RUN):
            ext[c, e + EDGE] = glu_n[c, pl.ds(2 * HEAD + e, S, stride=RUN), :].astype(BF16)

    rowsum[...] = jnp.zeros_like(rowsum)

    def convolve(c, source, first, count, start):
        for q in range(0, count, 4):
            some = range(min(4, count - q))
            acc = [None] * len(some)
            for k in range(TAPS):
                tap = tapb[c, k].astype(F32)
                for m in some:
                    v = source[c, start(q + m, k)].astype(F32) * tap
                    acc[m] = v if acc[m] is None else acc[m] + v
            for m in some:
                yield first + q + m, acc[m]

    @pl.loop(0, blocks)
    def _(c):
        for r, v in convolve(c, ext, 0, RUN, lambda r, k: r + k):
            convs[c, r] = v
            rowsum[r] += v

    lane = lax.broadcasted_iota(jnp.int32, (S, LANES), 1)

    def exchange(snd, rcv, index):
        return pltpu.make_async_remote_copy(
            snd, rcv, tp_send.at[index], tp_recv.at[index], device_id=other, device_id_type=MESH
        )

    def packed(pairs):
        tile = jnp.zeros((S, LANES), F32)
        for n, (one, two) in enumerate(pairs):
            tile = jnp.where(lane == 2 * n, one, jnp.where(lane == 2 * n + 1, two, tile))
        return tile

    def figures(first, count, index):
        for r in range(first, first + count):
            mean_l[r] = jnp.broadcast_to(jnp.sum(rowsum[r], axis=1, keepdims=True) * (1.0 / chans), (S, LANES))

        @pl.loop(first, first + count)
        def _(r):
            m = mean_l[r]
            acc = jnp.zeros((S, LANES), F32)
            for c in range(blocks):
                cent = convs[c, r] - m
                acc = acc + cent * cent
            rowdot[r] = acc

        stat_snd[index // 2] = packed(
            (mean_l[r], jnp.sum(rowdot[r], axis=1, keepdims=True)) for r in range(first, first + count)
        )
        return exchange(stat_snd.at[index // 2], stat_rcv.at[index // 2], index)

    def joined(first, count):
        own, far = stat_snd[first // RUN], stat_rcv[first // RUN]
        both = own + far
        diff = own - far
        for n in range(count):
            m, q = slice(2 * n, 2 * n + 1), slice(2 * n + 1, 2 * n + 2)
            spread = (both[:, q] + diff[:, m] * diff[:, m] * (chans / 2)) * (0.5 / chans)
            mean_l[first + n] = jnp.broadcast_to(0.5 * both[:, m], (S, LANES))
            rstd_s[first + n] = jnp.broadcast_to(lax.rsqrt(spread + EPS), (S, LANES))

    def swish(r, at):
        m, rs = mean_l[r], rstd_s[r]
        acc1 = jnp.zeros((S, LANES), F32)
        acc2 = jnp.zeros((S, LANES), F32)
        for c in range(blocks):
            lanes = slice(c * LANES, (c + 1) * LANES)
            normed = (convs[c, r] - m) * rs
            gain = gain_ref[lanes].reshape(1, LANES)
            half = normed * (0.5 * gain) + 0.5 * shift_ref[lanes].reshape(1, LANES)
            th = jnp.tanh(half)
            dpre = work[c, at, :] * (1.0 + th) * (1.0 + (half - half * th))
            dn = dpre * gain
            convs[c, r] = normed
            dnorm[c, r] = dn
            acc1 = acc1 + dn
            acc2 = acc2 + dn * normed
            prod = dpre * normed
            col[c, 0] += prod[:8] + prod[8:]
            col[c, 1] += dpre[:8] + dpre[8:]
        rowsum[r] = acc1
        rowdot[r] = acc2

    def sum_figures(first, count, index):
        sums_snd[index // 2] = packed(
            (jnp.sum(rowsum[r], axis=1, keepdims=True), jnp.sum(rowdot[r], axis=1, keepdims=True))
            for r in range(first, first + count)
        )
        copy = exchange(sums_snd.at[index // 2], sums_rcv.at[index // 2], index)
        copy.start()
        return copy

    def sums_joined(first, count):
        both = (sums_snd[first // RUN] + sums_rcv[first // RUN]) * (0.5 / chans)
        for n in range(count):
            rs = rstd_s[first + n]
            m1_s[first + n] = rs * both[:, 2 * n : 2 * n + 1]
            m2_s[first + n] = rs * both[:, 2 * n + 1 : 2 * n + 2]

    def dconv(c, r):
        return rstd_s[r] * dnorm[c, r] - m1_s[r] - convs[c, r] * m2_s[r]

    def body_at(r):
        return pl.ds(HEAD + r, S, stride=RUN)

    def head_at(r):
        return pl.ds(r, S, stride=HEAD // S)

    stat = figures(0, RUN, 0)

    @pl.when(first_x)
    def _():
        enter()

    stat.start()
    pl.semaphore_wait(round_sem.at[0], 2 + count(1))
    around(2, to_round(1))
    for i in (7, 8, 9):
        loads[i].wait()

    @pl.loop(0, blocks)
    def _(c):
        work[c] = 0.5 * cot_in[:, lanes_of(c)].astype(F32)

    stat.wait()
    joined(0, RUN)
    col[...] = jnp.zeros_like(col)

    @pl.loop(0, RUN)
    def _(r):
        swish(r, body_at(r))

    sums = sum_figures(0, RUN, 1)

    @pl.when(first_sp)
    def _():
        glu_n[:, :HEAD] = jnp.zeros((blocks, HEAD, LANES), F32)

    @pl.when(jnp.logical_not(first_sp))
    def _():
        for i in range(pieces):
            halo(i).wait_recv()

        @pl.loop(0, blocks)
        def _(c):
            glu_n[c, :HEAD] = halo_rcv[c].astype(F32)

    @pl.loop(0, blocks)
    def _(c):
        for e in range(-EDGE, 2):
            hext[c, e + EDGE] = glu_n[c, pl.ds(HEAD + e, S, stride=2), :].astype(BF16)

    @pl.loop(0, blocks // 2)
    def _(n):
        acc = [None] * 4
        for k in range(TAPS):
            for b in range(2):
                tap = tapb[2 * n + b, k].astype(F32)
                for r in range(2):
                    v = hext[2 * n + b, r + k].astype(F32) * tap
                    m = 2 * b + r
                    acc[m] = v if acc[m] is None else acc[m] + v
        for r in range(2):
            convs[2 * n, RUN + r] = acc[r]
            convs[2 * n + 1, RUN + r] = acc[2 + r]
            v = acc[r] + acc[2 + r]
            rowsum[RUN + r] = jnp.where(n == 0, v, rowsum[RUN + r] + v)

    head_stat = figures(RUN, 2, 2)
    head_stat.start()
    sums.wait()
    pl.semaphore_wait(round_sem.at[1], count(2))
    to_round(2)((lax.rem(z + nz // 2, nz), y, x, core))
    sums_joined(0, RUN)

    @pl.loop(0, blocks)
    def _(c):
        for r in range(RUN):
            d = dconv(c, r)
            dce[c, r] = d.astype(BF16)
            dconv_n[c, body_at(r), :] = d

    head_stat.wait()
    joined(RUN, 2)
    for r in range(2):
        swish(RUN + r, head_at(r))
    head_sums = sum_figures(RUN, 2, 3)
    sub = lax.broadcasted_iota(jnp.int32, (8, LANES), 0)
    for q in range(shards - 4 * blocks):
        rows = jnp.zeros((8, LANES), F32)
        for c in range(8 * q, min(8 * q + 8, blocks)):
            rows = jnp.where(sub == c % 8, jnp.sum(col[c, 1], axis=0, keepdims=True), rows)
        part[4 * blocks + q] = rows.astype(BF16)
    def correlate(c, rows, store):
        for q in range(8):
            ks = [k for k in range(q * 4, q * 4 + 4) if k < TAPS]
            acc = [None] * len(ks)
            for r in rows:
                d = (dce[c, r] if r < RUN else hdce[c, r - RUN]).astype(F32)
                for m, k in enumerate(ks):
                    g = ext[c, k + r] if r < RUN else hext[c, k + r - RUN]
                    v = g.astype(F32) * d
                    acc[m] = v if acc[m] is None else acc[m] + v
            for m, k in enumerate(ks):
                store(pl.ds(9 * k, 8), acc[m][:8] + acc[m][8:])

    @pl.loop(0, blocks)
    def _(c):
        def store(at, v):
            red[c, at, :] = v

        correlate(c, range(RUN - 2), store)

    head_sums.wait()
    sums_joined(RUN, 2)

    @pl.loop(0, blocks)
    def _(c):
        for r in range(2):
            d = dconv(c, RUN + r)
            hdce[c, r] = d.astype(BF16)
            dconv_n[c, head_at(r), :] = d
        back_snd[c] = dconv_n[c, :HEAD].astype(BF16)

    back = pltpu.make_async_remote_copy(
        back_snd, back_rcv, halo_send.at[pieces], halo_recv.at[pieces], device_id=behind, device_id_type=MESH
    )

    @pl.when(jnp.logical_not(first_sp))
    def _():
        back.start()


    @pl.loop(0, blocks)
    def _(c):
        def store(at, v):
            red[c, at, :] += v

        correlate(c, range(RUN - 2, S), store)
        red[c, pl.ds(9 * TAPS, 8), :] = col[c, 0]
        for g in range(4):
            rows = red[c, pl.ds(72 * g, 8, stride=9), :]
            for s in range(1, 8):
                rows = rows + red[c, pl.ds(72 * g + s, 8, stride=9), :]
            part[4 * c + g] = rows.astype(BF16)

    pl.semaphore_wait(round_sem.at[2], 1)

    def shard(index):
        return pl.ds(index * per, per)

    for device in others:
        owner = device[0] * ny + device[1]

        @pl.when(owner < owners)
        def _():
            pltpu.make_async_remote_copy(
                part.at[shard(owner)],
                part_rcv.at[shard(mine)],
                red_send.at[0],
                red_recv.at[0],
                device_id=device,
                device_id_type=MESH,
            ).start()

    def wait_all(ref, count, sem):
        some = ref.at[pl.ds(0, count * per)]
        pltpu.make_async_copy(some, some, sem).wait()

    @pl.when(mine < owners)
    def _():
        part_rcv[shard(mine)] = part[shard(mine)]
        wait_all(part_rcv, plane - 1, red_recv.at[0])
        sums8 = part_rcv[pl.ds(0, per)].astype(F32)
        for j in range(1, plane):
            sums8 = sums8 + part_rcv[pl.ds(j * per, per)].astype(F32)
        line_snd[...] = sums8
        line_rcv[shard(x)] = sums8
        for device in line:
            pltpu.make_async_remote_copy(
                line_snd,
                line_rcv.at[shard(x)],
                red_send.at[1],
                red_recv.at[1],
                device_id=device,
                device_id_type=MESH,
            ).start()
        wait_all(line_rcv, nx - 1, red_recv.at[1])
        sums8 = line_rcv[pl.ds(0, per)]
        for j in range(1, nx):
            sums8 = sums8 + line_rcv[pl.ds(j * per, per)]
        full_snd[...] = sums8.astype(BF16)
        full_rcv[shard(mine)] = sums8.astype(BF16)
        for device in others:
            pltpu.make_async_remote_copy(
                full_snd,
                full_rcv.at[shard(mine)],
                red_send.at[2],
                red_recv.at[2],
                device_id=device,
                device_id_type=MESH,
            ).start()


    @pl.when(last_sp)
    def _():
        dconv_n[:, ROWS:] = jnp.zeros((blocks, HEAD, LANES), F32)

    @pl.when(jnp.logical_not(last_sp))
    def _():
        back.wait_recv()

        @pl.loop(0, blocks)
        def _(c):
            dconv_n[c, ROWS:] = back_rcv[c].astype(F32)

    @pl.loop(0, blocks)
    def _(c):
        for e in range(RUN, RUN + EDGE):
            dce[c, e] = dconv_n[c, body_at(e), :].astype(BF16)
        for e in range(2, HEAD):
            hdce[c, e] = dconv_n[c, head_at(e), :].astype(BF16)

    @pl.loop(0, blocks)
    def _(c):
        for r, v in convolve(c, dce, 0, RUN, lambda r, k: r + EDGE - k):
            work[c, body_at(r), :] = v
        for r, v in convolve(c, hdce, 0, 2, lambda r, k: r + EDGE - k):
            work[c, head_at(r), :] = v

    @pl.loop(0, blocks)
    def _(c):
        sv = sg[c]
        first = work[c] * sv
        ag_out[:, lanes_of(c)] = first.astype(BF16)
        gg_out[:, lanes_of(c)] = (first * a_in[:, lanes_of(c)].astype(F32) * (1.0 - sv)).astype(BF16)

    @pl.when(mine < owners)
    def _():
        wait_all(full_rcv, owners - 1, red_recv.at[2])

    @pl.when(mine >= owners)
    def _():
        wait_all(full_rcv, owners, red_recv.at[2])

    for c in range(blocks):
        lanes = slice(c * LANES, (c + 1) * LANES)
        for g in range(4):
            rows = full_rcv[4 * c + g].astype(F32)
            if g < 3:
                tg_ref[8 * g : 8 * g + 8, lanes] = rows
            else:
                tg_ref[24:TAPS, lanes] = rows[:7]
                gng_ref[lanes] = rows[7:8].reshape(LANES)
        row = full_rcv[4 * blocks + c // 8].astype(F32)[c % 8 : c % 8 + 1]
        shg_ref[lanes] = row.reshape(LANES)


    @pl.when(jnp.logical_not(last_sp))
    def _():
        for i in range(pieces):
            halo(i).wait_send()

    @pl.when(jnp.logical_not(first_sp))
    def _():
        back.wait_send()

    @pl.when(mine < owners)
    def _():
        wait_all(part, owners - 1, red_send.at[0])
        wait_all(line_rcv, nx - 1, red_send.at[1])
        wait_all(part_rcv, plane - 1, red_send.at[2])

    @pl.when(mine >= owners)
    def _():
        wait_all(part, owners, red_send.at[0])


def put_out(*refs):
    *refs, sem = refs
    count = len(refs) // 2
    copies = [pltpu.make_async_copy(refs[i], refs[count + i], sem.at[i]) for i in range(count)]
    for copy in copies:
        copy.start()
    for copy in copies:
        copy.wait()


def body(sizes, proj_a, proj_gate, taps, norm_gain, norm_shift, cotangent):
    rows, chans = proj_a.shape
    blocks = chans // LANES
    nz, ny, nx = sizes
    plane = nz * ny
    shards = 4 * blocks + -(-blocks // 8)
    per = -(-shards // plane)
    assert shards % per == 0
    hbm = pl.BlockSpec(memory_space=pltpu.HBM)
    vmem = pl.BlockSpec(memory_space=pltpu.VMEM)
    tile = (S, S, LANES)
    edge = (blocks, 32, LANES)
    shapes = (
        jax.ShapeDtypeStruct((rows, chans), BF16),
        jax.ShapeDtypeStruct((rows, chans), BF16),
        jax.ShapeDtypeStruct((TAPS, chans), F32),
        jax.ShapeDtypeStruct((chans,), F32),
        jax.ShapeDtypeStruct((chans,), F32),
    )
    outs = pl.pallas_call(
        functools.partial(kernel, sizes),
        out_shape=tuple(pltpu.VMEM(shape.shape, shape.dtype) for shape in shapes),
        in_specs=[hbm] * 6,
        out_specs=(vmem,) * 5,
        scratch_shapes=[
            pltpu.VMEM((rows, chans), BF16),
            pltpu.VMEM((rows, chans), BF16),
            pltpu.VMEM((rows, chans), BF16),
            pltpu.VMEM((32, chans), BF16),
            pltpu.VMEM((32, chans), BF16),
            pltpu.VMEM((blocks, rows, LANES), F32),
            pltpu.VMEM((blocks, HEAD + rows, LANES), F32),
            pltpu.VMEM((blocks, rows, LANES), F32),
            pltpu.VMEM((blocks, rows + HEAD, LANES), F32),
            pltpu.VMEM((blocks, EDGE + RUN, S, LANES), BF16),
            pltpu.VMEM((blocks, EDGE + 2, S, LANES), BF16),
            pltpu.VMEM((blocks, EDGE + RUN, S, LANES), BF16),
            pltpu.VMEM((blocks, EDGE + 2, S, LANES), BF16),
            pltpu.VMEM((blocks, TAPS, S, LANES), BF16),
            pltpu.VMEM((blocks, *tile), F32),
            pltpu.VMEM((blocks, *tile), F32),
            pltpu.VMEM(tile, F32),
            pltpu.VMEM(tile, F32),
            pltpu.VMEM(tile, F32),
            pltpu.VMEM(tile, F32),
            pltpu.VMEM(tile, F32),
            pltpu.VMEM(tile, F32),
            pltpu.VMEM((2, S, LANES), F32),
            pltpu.VMEM((2, S, LANES), F32),
            pltpu.VMEM((2, S, LANES), F32),
            pltpu.VMEM((2, S, LANES), F32),
            pltpu.VMEM(edge, BF16),
            pltpu.VMEM(edge, BF16),
            pltpu.VMEM(edge, BF16),
            pltpu.VMEM(edge, BF16),
            pltpu.VMEM((blocks, 2, 8, LANES), F32),
            pltpu.VMEM((blocks, 9 * 32, LANES), F32),
            pltpu.VMEM((shards, 8, LANES), BF16),
            pltpu.VMEM((plane * per, 8, LANES), BF16),
            pltpu.VMEM((per, 8, LANES), F32),
            pltpu.VMEM((nx * per, 8, LANES), F32),
            pltpu.VMEM((per, 8, LANES), BF16),
            pltpu.VMEM((shards, 8, LANES), BF16),
            pltpu.VMEM((chans,), F32),
            pltpu.VMEM((chans,), F32),
            pltpu.VMEM((TAPS, chans), BF16),
            pltpu.SemaphoreType.DMA((10,)),
            pltpu.SemaphoreType.DMA((4,)),
            pltpu.SemaphoreType.DMA((4,)),
            pltpu.SemaphoreType.DMA((2,)),
            pltpu.SemaphoreType.DMA((2,)),
            pltpu.SemaphoreType.DMA((3,)),
            pltpu.SemaphoreType.DMA((3,)),
            pltpu.SemaphoreType.REGULAR((3,)),
        ],
        compiler_params=pltpu.CompilerParams(
            collective_id=0, has_side_effects=True, vmem_limit_bytes=64_000_000
        ),
    )(proj_a, proj_gate, cotangent, taps, norm_gain, norm_shift)
    return pl.pallas_call(
        put_out,
        out_shape=shapes,
        in_specs=[vmem] * 5,
        out_specs=(hbm,) * 5,
        scratch_shapes=[pltpu.SemaphoreType.DMA((5,))],
        compiler_params=pltpu.CompilerParams(vmem_limit_bytes=16_000_000),
    )(*outs)


def solution(mesh):
    sizes = (8, 8, 4)
    torus = Mesh(mesh.devices.reshape(*sizes, mesh.shape["tp"]), (*SP, "tp"))
    return jax.shard_map(
        functools.partial(body, sizes),
        mesh=torus,
        in_specs=(P(SP, "tp"), P(SP, "tp"), P(None, "tp"), P("tp"), P("tp"), P(SP, "tp")),
        out_specs=(P(SP, "tp"), P(SP, "tp"), P(None, "tp"), P("tp"), P("tp")),
        check_vma=False,
    )
```
